32 devices in a mesh: grp: 2 (over y), sp: 4 (over z), dp: 4 (over x, core).
Axes of the slice: x: 2, y: 2, z: 4, core: 2. Of those that a mesh axis runs over, the one named last changes fastest.
Arguments:
- tokens: bfloat16 [8, 640, 2048], P(('grp', 'dp'), 'sp'), parts along dimension 0, may hold values from -6 to 6
- query_weight: bfloat16 [2048, 1024], P('dp'), may hold values from -0.125 to 0.125
- key_weight: bfloat16 [2048, 256], P('dp'), may hold values from -0.125 to 0.125
- value_weight: bfloat16 [2048, 256], P('dp'), may hold values from -0.125 to 0.125
- out_weight: bfloat16 [1024, 2048], P(None, 'dp'), may hold values from -0.1875 to 0.1875
- query_gain: float32 [64], replicated, may hold values from 0.28 to 6
- key_gain: float32 [64], replicated, may hold values from 0.28 to 6
Outputs:
- mixed: bfloat16 [8, 640, 2048], P(('grp', 'dp'), 'sp'), parts along dimension 0
The draws below stay inside these ranges and needn't reach their ends.
There are 2 independent parts, one for each index of `grp`. The reference program is written for one: setup_inputs(seed, part) draws one part's arguments, and reference() takes and returns one part's arrays. A program takes and returns all parts, laid end to end along the dimension named above; an argument that names none is the same for every part. Nothing has to cross between parts.
All inputs are finite; a program needn't handle non-finite values.
Results may differ from the reference program's by a relative error of at most 0.006.
The reference program's roundings to bfloat16 on the way count: a program that leaves them out, or rounds other values in their place, can miss the bound.
Values may be sent and summed in bfloat16 or wider, within the bound.
A program may use at most 64 MiB of HBM per device.

```python
import jax
import jax.numpy as jnp
from jax import lax

D = 2048
HEADS = 16
KV_HEADS = 4
HEAD_DIM = 64
GRID_W = 64
SEQ_LEN = 640
SEQS = 4


def gain_values(key):
    return 1.0 + 0.18 * jnp.clip(jax.random.normal(key, (HEAD_DIM,), jnp.float32), -4.0, 4.0)


def draw_query_gain(key, part):
    return gain_values(jax.random.fold_in(key, 11))


def draw_key_gain(key, part):
    return gain_values(jax.random.fold_in(key, 23))


def level_of(rng, dims, split, least, largest):
    factor_of, own = 1.0, jax.random.fold_in(rng, 6)
    for position, blocks in split:
        steps = jnp.exp(jax.random.uniform(jax.random.fold_in(own, position), (blocks,), jnp.float32, least / len(split), largest / len(split)))
        factor_of = factor_of * jnp.repeat(steps, dims[position] // blocks).reshape([-1 if axis == position else 1 for axis in range(len(dims))])
    return factor_of


def gaussian(rng, shape, spread, bound, pieces=(), kind=jnp.bfloat16):
    values = jax.random.normal(rng, shape, jnp.float32) * spread
    if len(pieces) > 0:
        values = level_of(rng, shape, pieces, -0.22, 0.18) * values
    return jnp.clip(values, min=-bound, max=bound).astype(kind)


def setup_inputs(seed: int = 0, part: int = 0) -> dict:
    splits = jax.random.split(jax.random.key(seed), 8)
    part_splits = jax.random.split(jax.random.fold_in(splits[7], part), 8)
    tokens = gaussian(part_splits[0], (SEQS, SEQ_LEN, D), 1.0, 6.0, ((0, 4), (1, 4)))
    query_weight = gaussian(splits[1], (D, HEADS * HEAD_DIM), D ** -0.5, 0.125, ((0, 4),))
    key_weight = gaussian(splits[2], (D, KV_HEADS * HEAD_DIM), D ** -0.5, 0.125, ((0, 4),))
    value_weight = gaussian(splits[3], (D, KV_HEADS * HEAD_DIM), D ** -0.5, 0.125, ((0, 4),))
    out_weight = gaussian(splits[4], (HEADS * HEAD_DIM, D), (HEADS * HEAD_DIM) ** -0.5, 0.1875, ((1, 4),))
    query_gain = draw_query_gain(jax.random.fold_in(splits[7], 71), part)
    key_gain = draw_key_gain(jax.random.fold_in(splits[7], 71), part)
    return dict(tokens=tokens, query_weight=query_weight, key_weight=key_weight, value_weight=value_weight, out_weight=out_weight, query_gain=query_gain, key_gain=key_gain)


theta_base = 10000.0
norm_eps = 1e-06

def rotary_tables(positions):
    quarter = HEAD_DIM // 4
    inverse = theta_base ** (-jnp.arange(quarter, dtype=jnp.float32) / quarter)
    grid_rows = (positions // GRID_W).astype(jnp.float32)
    grid_cols = (positions % GRID_W).astype(jnp.float32)
    angles = jnp.concatenate([grid_rows[:, None] * inverse, grid_cols[:, None] * inverse], axis=-1)
    return (jnp.cos(angles), jnp.sin(angles))

def norm_rotate(raw, gain, cosine, sine):
    scaled = raw * lax.rsqrt(lax.optimization_barrier(jnp.mean(raw * raw, axis=-1, keepdims=True)) + norm_eps) * gain
    half = HEAD_DIM // 2
    first_half = scaled[..., :half]
    second_half = scaled[..., half:]
    cosine = cosine[:, None, :]
    sine = sine[:, None, :]
    turned = jnp.concatenate([first_half * cosine - second_half * sine, second_half * cosine + first_half * sine], axis=-1)
    return turned.astype(jnp.bfloat16)

def reference(tokens, query_weight, key_weight, value_weight, out_weight, query_gain, key_gain):
    length = tokens.shape[1]
    per_kv = HEADS // KV_HEADS
    cosine, sine = rotary_tables(jnp.arange(length, dtype=jnp.int32))
    scale = HEAD_DIM ** (-0.5)

    def one_sequence(rows_in):
        raw_q = jnp.dot(rows_in, query_weight, preferred_element_type=jnp.float32).reshape(length, HEADS, HEAD_DIM)
        raw_k = jnp.dot(rows_in, key_weight, preferred_element_type=jnp.float32).reshape(length, KV_HEADS, HEAD_DIM)
        values = jnp.dot(rows_in, value_weight, preferred_element_type=jnp.float32).astype(jnp.bfloat16)
        queries = norm_rotate(raw_q, query_gain, cosine, sine)
        keys = norm_rotate(raw_k, key_gain, cosine, sine)
        query_heads = queries.reshape(length, KV_HEADS, per_kv, HEAD_DIM).transpose(1, 0, 2, 3)
        key_heads = keys.transpose(1, 0, 2)
        value_heads = values.reshape(length, KV_HEADS, HEAD_DIM).transpose(1, 0, 2)

        def one_head(operands):
            head_q, head_k, head_v = operands
            scores = jnp.einsum('qgd,sd->gqs', head_q.astype(jnp.float32), head_k.astype(jnp.float32)) * scale
            top = lax.optimization_barrier(jnp.max(scores, axis=-1, keepdims=True))
            weights = jnp.exp(scores - top)
            probs = (weights / lax.optimization_barrier(jnp.sum(weights, axis=-1, keepdims=True))).astype(jnp.bfloat16)
            return jnp.einsum('gqs,sd->qgd', probs.astype(jnp.float32), head_v.astype(jnp.float32)).astype(jnp.bfloat16)
        attended = lax.map(one_head, (query_heads, key_heads, value_heads))
        attended = attended.transpose(1, 0, 2, 3).reshape(length, HEADS * HEAD_DIM)
        return jnp.dot(attended, out_weight, preferred_element_type=jnp.float32).astype(jnp.bfloat16)
    return lax.map(one_sequence, tokens)
```

```python
import functools
import math

import jax
import jax.numpy as jnp
from jax import lax
from jax.experimental import pallas as pl
from jax.experimental.pallas import tpu as pltpu
from jax.sharding import PartitionSpec as P

HEADS = 16
KV_HEADS = 4
HEAD_DIM = 64
GRID_W = 64
LANES = 128

theta_base = 10000.0
norm_eps = 1e-06

BF = jnp.bfloat16
F32 = jnp.float32
MESH = pl.DeviceIdType.MESH


def rotary_tables(start, rows):
    quarter = HEAD_DIM // 4
    lane = lax.broadcasted_iota(jnp.int32, (rows, LANES), 1)
    position = start + lax.broadcasted_iota(jnp.int32, (rows, LANES), 0)
    step = lax.rem(lane, quarter).astype(F32)
    inverse = jnp.exp(step * (-math.log(theta_base) / quarter))
    grid_row = lax.div(position, GRID_W)
    grid_col = lax.rem(position, GRID_W)
    place = jnp.where(lax.rem(lane, 2 * quarter) < quarter, grid_row, grid_col).astype(F32)
    angles = place * inverse
    sine = jnp.sin(angles)
    return jnp.cos(angles), jnp.where(lax.rem(lane, HEAD_DIM) < HEAD_DIM // 2, -sine, sine)


def dot(a, b):
    return jnp.dot(a, b, preferred_element_type=F32)


def kernel(n, groups, seqs, route, xlist, ylist, zlist, cq, co, tok_h, wk, wv, wq, wo, gq_h, gk_h, out,
           fk, fv, fq, fo, tok, gq, gk, cos, sin, kv, acc_k, acc_v, acc_q, qs, att,
           ls, os_, or_, xs, xr, ys, yr, zs, zr, cs, cr, hs, hr, fs):
    d = lax.axis_index("dp")
    g = lax.axis_index("grp")
    s = lax.axis_index("sp")
    chips = n // 2
    mate = d + 1 - 2 * lax.rem(d, 2)
    full = (fk, fv, fq, fo)
    rows = tok.shape[0]

    loads = []
    for i, (src, dst) in enumerate(((wk, fk.at[d]), (wv, fv.at[d]), (tok_h, tok), (wq, fq.at[d]), (wo, fo.at[d]),
                                    (gq_h, gq), (gk_h, gk))):
        copy = pltpu.make_async_copy(src, dst, ls.at[i])
        copy.start()
        loads.append(copy)

    def hop(j):
        return lax.rem(d + 2 * j, n)

    def back(dev, j):
        return lax.rem(dev + n - 2 * j, n)

    def other(i):
        return i + 1 - 2 * lax.rem(i, 2)

    def inside(i):
        return (i >= 0) & (i < seqs)

    def near(i):
        return jnp.clip(i, 0, seqs - 1)

    e = lax.rem(s, 2)
    colors = (2 * g + e, 2 * other(g) + e, 2 * g + other(e), 2 * other(g) + other(e))
    offsets = (2, -2, 1, -1)

    barrier = pltpu.get_barrier_semaphore()
    for j in range(1, chips):
        pl.semaphore_signal(barrier, inc=1, device_id={"dp": hop(j)}, device_id_type=MESH)
    for i in range(1, groups):
        pl.semaphore_signal(barrier, inc=1, device_id={"grp": lax.rem(g + i, groups)}, device_id_type=MESH)
    count = jnp.int32(chips - 1 + groups - 1 + 1)
    for o in offsets:
        def greet(o=o):
            pl.semaphore_signal(barrier, inc=1, device_id={"sp": near(s + o)}, device_id_type=MESH)
        pl.when(inside(s + o))(greet)
        count = count + inside(s + o).astype(jnp.int32)
    pl.semaphore_signal(barrier, inc=1, device_id={"dp": mate}, device_id_type=MESH)

    cos[...], sin[...] = rotary_tables(s * rows, rows)

    waits = []

    def remote(src, dst, ssem, rsem, where):
        return pltpu.make_async_remote_copy(
            src_ref=src, dst_ref=dst, send_sem=ssem, recv_sem=rsem, device_id=where, device_id_type=MESH)

    def arrive(dst, ssem, rsem):
        remote(dst, dst, ssem, rsem, {"dp": mate}).wait_recv()

    pieces = [(0, 0), (1, 0)] + [(2, c) for c in range(cq)] + [(3, c) for c in range(co)]
    cuts = (1, 1, cq, co)

    def part(owner, p, start, blocks):
        kind, cut = pieces[p]
        quarter = full[kind].shape[1] // 4
        width = full[kind].shape[2] // cuts[kind]
        ref = full[kind].at[owner]
        if isinstance(start, int):
            return ref.at[pl.ds(start * quarter, blocks * quarter), pl.ds(cut * width, width)]
        return ref.at[pl.ds(pl.multiple_of(start * quarter, 16), blocks * quarter), pl.ds(cut * width, width)]

    def held(owner, p, rel):
        return part(owner, p, colors[rel], 1)

    for copy in loads:
        copy.wait()
    pl.semaphore_wait(barrier, count)

    def x_send(index):
        p, rel = xlist[index]
        for j in range(1, chips):
            here = held(d, p, rel)
            remote(here, here, xs.at[j - 1, p], xr.at[j - 1, index], {"dp": hop(j)}).start()

    def own_send(kind):
        here = full[kind].at[d]
        remote(here, here, os_.at[kind], or_.at[kind], {"dp": mate}).start()

    ahead = 3
    for index in range(ahead):
        x_send(index)
    for kind in range(4):
        own_send(kind)
    for index in range(ahead, len(xlist)):
        x_send(index)

    def step(p, rel):
        way = route[p, rel]
        table, ssem, rsem = {"x": (xlist, xs, xr), "y": (ylist, ys, yr), "z": (zlist, zs, zr)}[way]
        for j in range(1, chips):
            here = held(back(d, j), p, rel)
            arrive(here, ssem.at[j - 1, 0], rsem.at[j - 1, table.index((p, rel))])
            if rel in (0, 1) and route[p, rel + 2] == "z":
                i = zlist.index((p, rel + 2))
                remote(here, here, zs.at[j - 1, zsend.index(p)], zr.at[j - 1, i], {"sp": other(s)}).start()
            if rel in (0, 2) and route[p, rel + 1] == "y":
                i = ylist.index((p, rel + 1))
                remote(here, here, ys.at[j - 1, p], yr.at[j - 1, i], {"grp": other(g)}).start()
            remote(here, here, cs.at[j - 1, p], cr.at[j - 1, p], {"dp": mate}).start()

    zsend = sorted({p for p, _ in zlist})

    def step_c(p):
        for j in range(1, chips):
            arrive(part(back(mate, j), p, 0, 4), cs.at[j - 1, p], cr.at[j - 1, p])

    def step_own(kind):
        arrive(full[kind].at[mate], os_.at[kind], or_.at[kind])

    def drain():
        for kind in range(4):
            here = full[kind].at[d]
            remote(here, here, os_.at[kind], or_.at[kind], {"dp": mate}).wait_send()
        for j in range(1, chips):
            for p in range(len(pieces)):
                for table, sem in ((xlist, xs.at[j - 1, p]), (ylist, ys.at[j - 1, p]),
                                   (zlist, zs.at[j - 1, zsend.index(p)] if p in zsend else None)):
                    blocks = len([1 for q, _ in table if q == p])
                    if blocks:
                        here = part(d, p, 0, blocks)
                        remote(here, here, sem, xr.at[0, 0], {"dp": mate}).wait_send()
                here = part(back(d, j), p, 0, 4)
                remote(here, here, cs.at[j - 1, p], cr.at[j - 1, p], {"dp": mate}).wait_send()
        for i, o in enumerate(offsets):
            here = kv.at[s]
            pl.when(inside(s + o))(remote(here, here, hs.at[i], hr.at[0, 0], {"dp": mate}).wait_send)
        for i, (way, k, o) in enumerate(relays):
            here = kv.at[near(s - way * k)]
            pl.when(inside(s - way * k) & inside(s + way * o))(
                remote(here, here, fs.at[i], hr.at[0, 0], {"dp": mate}).wait_send)

    relays = [(way, k, o) for way in (1, -1) for k in range(2, seqs, 2) for o in (1, 2) if k + o < seqs]
    half = kv.shape[2] // 2

    def slot(i, which):
        return kv.at[i, :, pl.ds(which * half, half)]

    def spread(which):
        for i, o in enumerate(offsets):
            here = slot(s, which)
            pl.when(inside(s + o))(
                remote(here, here, hs.at[i], hr.at[s, which], {"sp": near(s + o)}).start)

    def collect(which, k):
        for way in (1, -1):
            source = near(s - way * k)
            here = slot(source, which)

            def take(here=here, source=source):
                arrive(here, hs.at[0], hr.at[source, which])
            pl.when(inside(s - way * k))(take)
            for i, (w, kk, o) in enumerate(relays):
                if w == way and kk == k:
                    pl.when(inside(s - way * k) & inside(s + way * o))(
                        remote(here, here, fs.at[i], hr.at[source, which], {"sp": near(s + way * o)}).start)

    depth = fq.shape[1]

    def columns(owner):
        return pl.ds(pl.multiple_of(owner * depth, LANES), depth)

    def first(acc, ref):
        acc[...] = dot(tok[:, columns(d)], ref[d])

    def more(acc, ref, owner):
        acc[...] += dot(tok[:, columns(owner)], ref[owner])

    first(acc_k, fk)
    first(acc_v, fv)
    first(acc_q, fq)

    lane = lax.broadcasted_iota(jnp.int32, (rows, LANES), 1)
    low_half = lax.rem(lane, HEAD_DIM) < HEAD_DIM // 2
    low_head = lane < HEAD_DIM
    square_r = lax.broadcasted_iota(jnp.int32, (LANES, LANES), 0)
    square_c = lax.broadcasted_iota(jnp.int32, (LANES, LANES), 1)
    same_head = jnp.where(square_r // HEAD_DIM == square_c // HEAD_DIM, 1.0, 0.0).astype(BF)

    gain_k = jnp.concatenate([gk[...]] * 2, axis=1)
    gain_q = jnp.concatenate([gq[...]] * 2, axis=1)

    def norm_rotate(raw, gain):
        sq = raw * raw
        high = sq.astype(BF)
        low = (sq - high.astype(F32)).astype(BF)
        total = dot(high, same_head) + dot(low, same_head)
        scaled = raw * lax.rsqrt(total * (1.0 / HEAD_DIM) + norm_eps) * gain
        other = jnp.where(low_half, pltpu.roll(scaled, LANES - HEAD_DIM // 2, 1),
                          pltpu.roll(scaled, HEAD_DIM // 2, 1))
        return scaled * cos[...] + other * sin[...]

    others = [(d, j) for j in range(1, chips)] + [(mate, j) for j in range(1, chips)]

    def finish_k():
        step_c(0)
        for dev, j in others:
            more(acc_k, fk, back(dev, j))
        for t in range(half // LANES):
            cols = pl.ds(t * LANES, LANES)
            kv[s, :, cols] = norm_rotate(acc_k[:, cols], gain_k).astype(BF)

    def finish_v():
        step_c(1)
        for dev, j in others:
            more(acc_v, fv, back(dev, j))
        kv[s, :, pl.ds(half, half)] = acc_v[...].astype(BF)

    tiles = fq.shape[2] // LANES
    group = HEADS // KV_HEADS

    def finish_q(cut):
        step_c(2 + cut)
        width = fq.shape[2] // cq
        cols = pl.ds(cut * width, width)
        for dev, j in others:
            owner = back(dev, j)
            acc_q[:, cols] += dot(tok[:, columns(owner)], fq[owner, :, cols])
        for t in range(cut * tiles // cq, (cut + 1) * tiles // cq):
            turned = norm_rotate(acc_q[:, pl.ds(t * LANES, LANES)], gain_q).astype(BF).astype(F32)
            turned = turned * HEAD_DIM ** (-0.5)
            swapped = pltpu.roll(turned, HEAD_DIM, 1)
            if (2 * t // group) % 2 == 0:
                one, two = jnp.where(low_head, turned, 0.0), jnp.where(low_head, swapped, 0.0)
            else:
                one, two = jnp.where(low_head, 0.0, swapped), jnp.where(low_head, 0.0, turned)
            qs[t, pl.ds(0, rows), :] = one.astype(BF)
            qs[t, pl.ds(rows, rows), :] = two.astype(BF)

    def attend(lo, hi):
        for t in range(lo, hi):
            h = 2 * t // group
            base = (h // 2) * LANES
            keys = kv[:, :, pl.ds(base, LANES)].reshape(seqs * rows, LANES)
            values = kv[:, :, pl.ds(half + base, LANES)].reshape(seqs * rows, LANES)
            scores = lax.dot_general(qs[t], keys, (((1,), (1,)), ((), ())), preferred_element_type=F32)
            top = jnp.max(scores, axis=-1, keepdims=True)
            weights = jnp.exp(scores - top)
            inverse = 1.0 / jnp.sum(weights, axis=-1, keepdims=True)
            mixed = dot((weights * inverse).astype(BF), values)
            one, two = mixed[:rows], mixed[rows:]
            if h % 2 == 0:
                two = pltpu.roll(two, HEAD_DIM, 1)
            else:
                one = pltpu.roll(one, HEAD_DIM, 1)
            att[:, pl.ds(t * LANES, LANES)] = jnp.where(low_head, one, two).astype(BF)

    def project(owner, lo, hi):
        width = fo.shape[2]
        size = (hi - lo) * (width // co)
        offset = lo * (width // co)
        out[:, pl.ds(pl.multiple_of(owner * width + offset, LANES), size)] = dot(
            att[...], fo[owner, :, pl.ds(offset, size)]).astype(BF)

    Q = [2 + c for c in range(cq)]
    O = [2 + cq + c for c in range(co)]
    q0, q1 = Q[0], Q[-1]

    def od(i, rel):
        if i < co:
            step(O[i], rel)

    step(0, 0)
    step(1, 0)
    step_own(0)
    more(acc_k, fk, mate)
    step_own(1)
    more(acc_v, fv, mate)
    step(0, 3)
    step(0, 1)
    step(0, 2)
    finish_k()
    spread(0)
    step(1, 1)
    step(1, 2)
    step(q0, 0)
    step_own(2)
    more(acc_q, fq, mate)
    step(1, 3)
    finish_v()
    spread(1)
    collect(0, 2)
    step(q0, 2)
    step(q0, 1)
    step(q1, 0)
    collect(1, 2)
    step(q0, 3)
    step(q1, 2)
    finish_q(0)
    od(0, 0)
    step(q1, 1)
    od(1, 0)
    [collect(0, k) for k in range(1, seqs) if k != 2]
    [collect(1, k) for k in range(1, seqs) if k != 2]
    od(2, 0)
    attend(0, tiles // 4)
    step(q1, 3)
    od(3, 0)
    od(0, 2)
    attend(tiles // 4, tiles // 2)
    od(0, 1)
    od(1, 2)
    finish_q(1)
    attend(tiles // 2, tiles * 3 // 4)
    od(1, 1)
    od(2, 2)
    od(1, 3)
    attend(tiles * 3 // 4, tiles)
    od(2, 1)
    od(3, 2)
    od(2, 3)
    project(d, 0, co)
    step_own(3)
    project(mate, 0, co)
    od(3, 1)
    od(3, 3)
    od(0, 3)
    [project(back(d, j), 0, co) for j in range(1, chips)]
    for p in O:
        step_c(p)
    for j in range(1, chips):
        project(back(mate, j), 0, co)
    drain()


def shards(n, groups, seqs, tokens, query_weight, key_weight, value_weight, out_weight, query_gain, key_gain):
    rows, width = tokens.shape[1], tokens.shape[2]
    local = tokens.reshape(rows, width)
    chips = n // 2
    kvw, qw = key_weight.shape[1], query_weight.shape[1]
    cq = 2
    co = max(1, min(4, out_weight.shape[1] // LANES))
    pieces = 2 + cq + co
    Q = range(2, 2 + cq)
    O = range(2 + cq, pieces)
    xlist = [(0, 0), (1, 0), (0, 3)] + [(p, r) for p in Q for r in (0, 2)] + [(p, 0) for p in O] + [
        (p, 3) for p in O[1:]]
    ylist = [(0, 1), (1, 1), (1, 3)] + [(p, r) for p in Q for r in (1, 3)] + [(p, 1) for p in O]
    zlist = [(0, 2), (1, 2)] + [(p, 2) for p in O] + [(O[0], 3)]
    route = {**{k: "x" for k in xlist}, **{k: "y" for k in ylist}, **{k: "z" for k in zlist}}
    zsends = len({p for p, _ in zlist})
    relays = 2 * len([1 for k in range(2, seqs, 2) for o in (1, 2) if k + o < seqs])
    dma = pltpu.SemaphoreType.DMA
    vmem = pl.BlockSpec(memory_space=pltpu.VMEM)
    hbm = pl.BlockSpec(memory_space=pltpu.HBM)
    result = pl.pallas_call(
        functools.partial(kernel, n, groups, seqs, route, xlist, ylist, zlist, cq, co),
        out_shape=pltpu.VMEM((rows, width), BF),
        in_specs=[hbm] * 7,
        out_specs=vmem,
        scratch_shapes=[
            pltpu.VMEM((n,) + key_weight.shape, BF),
            pltpu.VMEM((n,) + value_weight.shape, BF),
            pltpu.VMEM((n,) + query_weight.shape, BF),
            pltpu.VMEM((n,) + out_weight.shape, BF),
            pltpu.VMEM((rows, width), BF),
            pltpu.VMEM((1, HEAD_DIM), F32),
            pltpu.VMEM((1, HEAD_DIM), F32),
            pltpu.VMEM((rows, LANES), F32),
            pltpu.VMEM((rows, LANES), F32),
            pltpu.VMEM((seqs, rows, 2 * kvw), BF),
            pltpu.VMEM((rows, kvw), F32),
            pltpu.VMEM((rows, kvw), F32),
            pltpu.VMEM((rows, qw), F32),
            pltpu.VMEM((qw // LANES, 2 * rows, LANES), BF),
            pltpu.VMEM((rows, qw), BF),
            dma((7,)), dma((4,)), dma((4,)),
            dma((chips - 1, pieces)), dma((chips - 1, len(xlist))),
            dma((chips - 1, pieces)), dma((chips - 1, len(ylist))),
            dma((chips - 1, zsends)), dma((chips - 1, len(zlist))),
            dma((chips - 1, pieces)), dma((chips - 1, pieces)),
            dma((4,)), dma((seqs, 2)), dma((max(1, relays),)),
        ],
        compiler_params=pltpu.CompilerParams(
            collective_id=0, has_side_effects=True, vmem_limit_bytes=40 * 2 ** 20),
    )(*[pltpu.with_memory_space_constraint(a, pltpu.HBM) for a in (
        local, key_weight, value_weight, query_weight, out_weight,
        query_gain.reshape(1, HEAD_DIM), key_gain.reshape(1, HEAD_DIM))])
    return result.reshape(1, rows, width)


def solution(mesh):
    in_specs = (
        P(("grp", "dp"), "sp", None),
        P("dp", None),
        P("dp", None),
        P("dp", None),
        P(None, "dp"),
        P(),
        P(),
    )
    out_specs = P(("grp", "dp"), "sp", None)
    body = functools.partial(shards, mesh.shape["dp"], mesh.shape["grp"], mesh.shape["sp"])
    return jax.shard_map(body, mesh=mesh, in_specs=in_specs, out_specs=out_specs, check_vma=False)
```

```python
import functools
import math

import jax
import jax.numpy as jnp
from jax import lax
from jax.experimental import pallas as pl
from jax.experimental.pallas import tpu as pltpu
from jax.sharding import PartitionSpec as P

HEADS = 16
KV_HEADS = 4
HEAD_DIM = 64
GRID_W = 64
LANES = 128

theta_base = 10000.0
norm_eps = 1e-06

BF = jnp.bfloat16
F32 = jnp.float32
MESH = pl.DeviceIdType.MESH


def rotary_tables(start, rows):
    quarter = HEAD_DIM // 4
    lane = lax.broadcasted_iota(jnp.int32, (rows, LANES), 1)
    position = start + lax.broadcasted_iota(jnp.int32, (rows, LANES), 0)
    step = lax.rem(lane, quarter).astype(F32)
    inverse = jnp.exp(step * (-math.log(theta_base) / quarter))
    grid_row = lax.div(position, GRID_W)
    grid_col = lax.rem(position, GRID_W)
    place = jnp.where(lax.rem(lane, 2 * quarter) < quarter, grid_row, grid_col).astype(F32)
    angles = place * inverse
    sine = jnp.sin(angles)
    return jnp.cos(angles), jnp.where(lax.rem(lane, HEAD_DIM) < HEAD_DIM // 2, -sine, sine)


def dot(a, b):
    return jnp.dot(a, b, preferred_element_type=F32)

X_PIECES = ((0, 0, 0), (1, 0, 0), (2, 0, 0), (0, 0, 3), (2, 1, 0), (2, 3, 0), (2, 1, 2), (2, 2, 2), (3, 2, 0), (3, 1, 0), (3, 0, 2), (2, 2, 0), (3, 3, 1), (2, 2, 1), (3, 3, 2), (3, 1, 2), (3, 0, 0), (3, 3, 0), (3, 0, 1))
Y_PIECES = ((0, 0, 1), (1, 0, 1), (1, 0, 3), (2, 0, 1), (2, 0, 3), (2, 1, 1), (2, 1, 3), (2, 2, 3), (2, 3, 1), (2, 3, 3), (3, 0, 3), (3, 1, 1), (3, 2, 1), (3, 2, 3))
Z_PIECES = ((0, 0, 2), (1, 0, 2), (2, 0, 2), (2, 3, 2), (3, 1, 3), (3, 2, 2), (3, 3, 3))


def kernel(n, groups, seqs, route, xlist, ylist, zlist, cq, co, tok_h, wk, wv, wq, wo, gq_h, gk_h, out,
           fk, fv, fq, fo, tok, gq, gk, cos, sin, kv, acc_k, acc_v, acc_q, qs, att, probs,
           ls, os_, or_, xs, xr, ys, yr, zs, zr, cs, cr, hs, hr, fs, ready):
    d = lax.axis_index("dp")
    g = lax.axis_index("grp")
    s = lax.axis_index("sp")
    chips = n // 2
    mate = d + 1 - 2 * lax.rem(d, 2)
    full = (fk, fv, fq, fo)
    rows = tok.shape[0]

    loads = []
    for i, (src, dst) in enumerate(((wk, fk.at[d]), (wv, fv.at[d]), (tok_h, tok), (wq, fq.at[d]), (wo, fo.at[d]),
                                    (gq_h, gq), (gk_h, gk))):
        copy = pltpu.make_async_copy(src, dst, ls.at[i])
        copy.start()
        loads.append(copy)

    def hop(j):
        return lax.rem(d + 2 * j, n)

    def back(dev, j):
        return lax.rem(dev + n - 2 * j, n)

    def other(i):
        return i + 1 - 2 * lax.rem(i, 2)

    def inside(i):
        return (i >= 0) & (i < seqs)

    def near(i):
        return jnp.clip(i, 0, seqs - 1)

    e = lax.rem(s, 2)
    colors = (2 * g + e, 2 * other(g) + e, 2 * g + other(e), 2 * other(g) + other(e))
    offsets = (2, -2, 1, -1)

    barrier = pltpu.get_barrier_semaphore()
    for j in range(1, chips):
        pl.semaphore_signal(barrier, inc=1, device_id={"dp": hop(j)}, device_id_type=MESH)
    for i in range(1, groups):
        pl.semaphore_signal(barrier, inc=1, device_id={"grp": lax.rem(g + i, groups)}, device_id_type=MESH)
    count = jnp.int32(chips - 1 + groups - 1 + 1)
    for o in (1, -1):
        def greet(o=o):
            pl.semaphore_signal(barrier, inc=1, device_id={"sp": near(s + o)}, device_id_type=MESH)
        pl.when(inside(s + o))(greet)
        count = count + inside(s + o).astype(jnp.int32)
    pl.semaphore_signal(barrier, inc=1, device_id={"dp": mate}, device_id_type=MESH)

    cos[...], sin[...] = rotary_tables(s * rows, rows)

    waits = []

    def remote(src, dst, ssem, rsem, where):
        return pltpu.make_async_remote_copy(
            src_ref=src, dst_ref=dst, send_sem=ssem, recv_sem=rsem, device_id=where, device_id_type=MESH)

    def arrive(dst, ssem, rsem):
        remote(dst, dst, ssem, rsem, {"dp": mate}).wait_recv()

    pieces = [(0, 0), (1, 0)] + [(2, c) for c in range(cq)] + [(3, c) for c in range(co)]
    cuts = (1, 1, cq, co)

    shelf = [kind if kind < 2 else 2 + 2 * c // cq if kind == 2 else 4 for kind, c in pieces]

    def part(owner, p, start, blocks):
        kind, cut = pieces[p]
        quarter = full[kind].shape[1] // 4
        width = full[kind].shape[2] // cuts[kind]
        ref = full[kind].at[owner]
        if isinstance(start, int):
            return ref.at[pl.ds(start * quarter, blocks * quarter), pl.ds(cut * width, width)]
        return ref.at[pl.ds(pl.multiple_of(start * quarter, 16), blocks * quarter), pl.ds(cut * width, width)]

    def held(owner, p, rel):
        return part(owner, p, colors[rel], 1)

    for copy in loads:
        copy.wait()
    pl.semaphore_wait(barrier, count)

    for i, o in enumerate((1, -1)):
        def vouch(i=i, o=o):
            pl.semaphore_signal(ready.at[i], inc=1, device_id={"sp": near(s + o)}, device_id_type=MESH)
        pl.when(inside(s + o) & inside(s - o))(vouch)

    def x_send(index):
        p, rel = xlist[index]
        for j in range(1, chips):
            here = held(d, p, rel)
            remote(here, here, xs.at[j - 1, pieces[p][0]], xr.at[j - 1, index], {"dp": hop(j)}).start()

    def own_send(kind):
        here = full[kind].at[d]
        remote(here, here, os_.at[kind], or_.at[kind], {"dp": mate}).start()

    for index in range(4):
        x_send(index)
    for kind in range(4):
        own_send(kind)
    for index in range(4, len(xlist)):
        x_send(index)

    def step(p, rel):
        way = route[p, rel]
        table, ssem, rsem = {"x": (xlist, xs, xr), "y": (ylist, ys, yr), "z": (zlist, zs, zr)}[way]
        for j in range(1, chips):
            here = held(back(d, j), p, rel)
            arrive(here, ssem.at[j - 1, 0], rsem.at[j - 1, table.index((p, rel))])
            if rel in (0, 1) and route[p, rel + 2] == "z":
                i = zlist.index((p, rel + 2))
                remote(here, here, zs.at[j - 1, pieces[p][0]], zr.at[j - 1, i], {"sp": other(s)}).start()
            if rel in (0, 2) and route[p, rel + 1] == "y":
                i = ylist.index((p, rel + 1))
                remote(here, here, ys.at[j - 1, pieces[p][0]], yr.at[j - 1, i], {"grp": other(g)}).start()
            remote(here, here, cs.at[j - 1, pieces[p][0]], cr.at[j - 1, shelf[p]], {"dp": mate}).start()

    def step_c(kind, lo, hi):
        width = full[kind].shape[2] // cuts[kind]
        for j in range(1, chips):
            arrive(full[kind].at[back(mate, j), :, pl.ds(lo * width, (hi - lo) * width)],
                   cs.at[j - 1, kind], cr.at[j - 1, shelf[pieces.index((kind, lo))]])

    def step_own(kind):
        arrive(full[kind].at[mate], os_.at[kind], or_.at[kind])

    def drain():
        for kind in range(4):
            here = full[kind].at[d]
            remote(here, here, os_.at[kind], or_.at[kind], {"dp": mate}).wait_send()
        for j in range(1, chips):
            for kind in range(4):
                for table, sem in ((xlist, xs), (ylist, ys), (zlist, zs)):
                    blocks = len([1 for q, _ in table if pieces[q][0] == kind])
                    if blocks:
                        here = full[kind].at[d, pl.ds(0, blocks * (full[kind].shape[1] // 4) // cuts[kind])]
                        remote(here, here, sem.at[j - 1, kind], xr.at[0, 0], {"dp": mate}).wait_send()
                here = full[kind].at[d]
                remote(here, here, cs.at[j - 1, kind], cr.at[j - 1, 0], {"dp": mate}).wait_send()
        for i, o in enumerate(offsets):
            here = kv.at[s]
            pl.when(inside(s + o))(remote(here, here, hs.at[i], hr.at[0, 0], {"dp": mate}).wait_send)
        for i, (way, k, o) in enumerate(relays):
            here = kv.at[near(s - way * k)]
            pl.when(inside(s - way * k) & inside(s + way * o))(
                remote(here, here, fs.at[i], hr.at[0, 0], {"dp": mate}).wait_send)

    relays = [(way, k, o) for way in (1, -1) for k in range(2, seqs, 2) for o in (1, 2) if k + o < seqs]
    half = kv.shape[2] // 2

    def slot(i, which):
        return kv.at[i, :, pl.ds(which * half, half)]

    def met():
        for i, o in enumerate((1, -1)):
            def heard(i=i):
                pl.semaphore_wait(ready.at[i], 1)
            pl.when(inside(s - o) & inside(s - 2 * o))(heard)

    def spread(which):
        for i, o in enumerate(offsets):
            here = slot(s, which)
            pl.when(inside(s + o))(
                remote(here, here, hs.at[i], hr.at[s, which], {"sp": near(s + o)}).start)

    def onward(way, k):
        return functools.reduce(lambda a, b: a | b, [inside(s + way * o) for w, kk, o in relays if (w, kk) == (way, k)])

    def take(which, way, k):
        source = near(s - way * k)
        arrive(slot(source, which), hs.at[0], hr.at[source, which])

    def relay(which, k):
        for way in (1, -1):
            if not [1 for w, kk, o in relays if (w, kk) == (way, k)]:
                continue
            source = near(s - way * k)
            here = slot(source, which)
            pl.when(inside(s - way * k) & onward(way, k))(functools.partial(take, which, way, k))
            for i, (w, kk, o) in enumerate(relays):
                if (w, kk) == (way, k):
                    pl.when(inside(s - way * k) & inside(s + way * o))(
                        remote(here, here, fs.at[i], hr.at[source, which], {"sp": near(s + way * o)}).start)

    def collect(which):
        for k in range(1, seqs):
            for way in (1, -1):
                need = inside(s - way * k)
                if [1 for w, kk, o in relays if (w, kk) == (way, k)]:
                    need = need & jnp.logical_not(onward(way, k))
                pl.when(need)(functools.partial(take, which, way, k))

    depth = fq.shape[1]

    def columns(owner):
        return pl.ds(pl.multiple_of(owner * depth, LANES), depth)

    def first(acc, ref):
        acc[...] = dot(tok[:, columns(d)], ref[d])

    def more(acc, ref, owner):
        acc[...] += dot(tok[:, columns(owner)], ref[owner])

    first(acc_k, fk)
    first(acc_v, fv)
    first(acc_q, fq)

    lane = lax.broadcasted_iota(jnp.int32, (rows, LANES), 1)
    low_half = lax.rem(lane, HEAD_DIM) < HEAD_DIM // 2
    low_head = lane < HEAD_DIM
    square_r = lax.broadcasted_iota(jnp.int32, (LANES, LANES), 0)
    square_c = lax.broadcasted_iota(jnp.int32, (LANES, LANES), 1)
    same_head = jnp.where(square_r // HEAD_DIM == square_c // HEAD_DIM, 1.0, 0.0).astype(BF)

    gain_k = jnp.concatenate([gk[...]] * 2, axis=1)
    gain_q = jnp.concatenate([gq[...]] * 2, axis=1)

    def norm_rotate(raw, gain):
        sq = raw * raw
        high = sq.astype(BF)
        low = (sq - high.astype(F32)).astype(BF)
        total = dot(high, same_head) + dot(low, same_head)
        scaled = raw * lax.rsqrt(total * (1.0 / HEAD_DIM) + norm_eps) * gain
        other = jnp.where(low_half, pltpu.roll(scaled, LANES - HEAD_DIM // 2, 1),
                          pltpu.roll(scaled, HEAD_DIM // 2, 1))
        return scaled * cos[...] + other * sin[...]

    others = [(d, j) for j in range(1, chips)] + [(mate, j) for j in range(1, chips)]

    def finish_k():
        step_c(0, 0, 1)
        for dev, j in others:
            more(acc_k, fk, back(dev, j))
        for t in range(half // LANES):
            cols = pl.ds(t * LANES, LANES)
            kv[s, :, cols] = norm_rotate(acc_k[:, cols], gain_k).astype(BF)

    def finish_v():
        step_c(1, 0, 1)
        for dev, j in others:
            more(acc_v, fv, back(dev, j))
        kv[s, :, pl.ds(half, half)] = acc_v[...].astype(BF)

    tiles = fq.shape[2] // LANES
    group = HEADS // KV_HEADS

    def finish_q(part_):
        step_c(2, part_ * cq // 2, (part_ + 1) * cq // 2)
        width = fq.shape[2] // 2
        cols = pl.ds(part_ * width, width)
        for dev, j in others:
            owner = back(dev, j)
            acc_q[:, cols] += dot(tok[:, columns(owner)], fq[owner, :, cols])
        for t in range(part_ * tiles // 2, (part_ + 1) * tiles // 2):
            turned = norm_rotate(acc_q[:, pl.ds(t * LANES, LANES)], gain_q * HEAD_DIM ** (-0.5))
            swapped = pltpu.roll(turned, HEAD_DIM, 1)
            if (2 * t // group) % 2 == 0:
                one, two = jnp.where(low_head, turned, 0.0), jnp.where(low_head, swapped, 0.0)
            else:
                one, two = jnp.where(low_head, 0.0, swapped), jnp.where(low_head, 0.0, turned)
            qs[t, pl.ds(0, rows), :] = one.astype(BF)
            qs[t, pl.ds(rows, rows), :] = two.astype(BF)

    def softmax(h):
        base = (h // 2) * LANES
        keys = kv[:, :, pl.ds(base, LANES)].reshape(seqs * rows, LANES)
        lo, count = h * tiles // KV_HEADS, tiles // KV_HEADS
        asked = qs[lo:lo + count].reshape(count * 2 * rows, LANES)
        scores = lax.dot_general(asked, keys, (((1,), (1,)), ((), ())), preferred_element_type=F32)
        top = jnp.max(scores, axis=-1, keepdims=True)
        weights = jnp.exp(scores - top)
        inverse = 1.0 / jnp.sum(weights, axis=-1, keepdims=True)
        return (weights * inverse).astype(BF)

    def mix(h, weights):
        base = (h // 2) * LANES
        lo, count = h * tiles // KV_HEADS, tiles // KV_HEADS
        values = kv[:, :, pl.ds(half + base, LANES)].reshape(seqs * rows, LANES)
        mixed = dot(weights, values)
        for i in range(count):
            one, two = mixed[2 * i * rows:(2 * i + 1) * rows], mixed[(2 * i + 1) * rows:(2 * i + 2) * rows]
            if h % 2 == 0:
                two = pltpu.roll(two, HEAD_DIM, 1)
            else:
                one = pltpu.roll(one, HEAD_DIM, 1)
            att[:, pl.ds((lo + i) * LANES, LANES)] = jnp.where(low_head, one, two).astype(BF)

    def soft(h):
        probs[h] = softmax(h)

    def blend(h):
        mix(h, probs[h])

    def heads(h):
        mix(h, softmax(h))

    def project(owner, lo, hi):
        width = fo.shape[2]
        size = (hi - lo) * (width // co)
        offset = lo * (width // co)
        out[:, pl.ds(pl.multiple_of(owner * width + offset, LANES), size)] = dot(
            att[...], fo[owner, :, pl.ds(offset, size)]).astype(BF)

    Q = [2 + c for c in range(cq)]
    O = [2 + cq + c for c in range(co)]
    def q(i, rel):
        step(Q[i], rel)


    def od(i, rel):
        if i < co:
            step(O[i], rel)

    step(0, 0)
    step_own(0)
    more(acc_k, fk, mate)
    step(1, 0)
    step(0, 1)
    q(0, 0)
    step(1, 2)
    step(0, 2)
    step(0, 3)
    finish_k()
    met()
    spread(0)
    q(1, 0)
    q(3, 0)
    step(1, 3)
    q(1, 2)
    step(1, 1)
    q(1, 1)
    q(0, 2)
    step_own(1)
    more(acc_v, fv, mate)
    step_own(2)
    more(acc_q, fq, mate)
    finish_v()
    spread(1)
    relay(0, 2)
    q(3, 1)
    q(2, 2)
    q(3, 2)
    q(0, 1)
    q(1, 3)
    od(1, 0)
    q(2, 0)
    q(0, 3)
    od(2, 0)
    relay(1, 2)
    od(0, 2)
    finish_q(0)
    q(2, 3)
    q(2, 1)
    q(3, 3)
    collect(0)
    soft(0)
    od(3, 1)
    soft(1)
    od(1, 1)
    od(2, 2)
    finish_q(1)
    collect(1)
    blend(0)
    heads(2)
    od(0, 0)
    od(1, 2)
    od(2, 1)
    heads(3)
    od(3, 3)
    od(3, 0)
    od(2, 3)
    od(3, 2)
    blend(1)
    od(0, 1)
    od(0, 3)
    od(1, 3)
    project(d, 0, co)
    step_own(3)
    project(mate, 0, co)
    [project(back(d, j), 0, co) for j in range(1, chips)]
    step_c(3, 0, co)
    for j in range(1, chips):
        project(back(mate, j), 0, co)
    drain()


def shards(n, groups, seqs, tokens, query_weight, key_weight, value_weight, out_weight, query_gain, key_gain):
    rows, width = tokens.shape[1], tokens.shape[2]
    local = tokens.reshape(rows, width)
    chips = n // 2
    kvw, qw = key_weight.shape[1], query_weight.shape[1]
    cq = 4
    co = max(1, min(4, out_weight.shape[1] // LANES))
    pieces = 2 + cq + co
    index = {(0, 0): 0, (1, 0): 1, **{(2, c): 2 + c for c in range(cq)}, **{(3, c): 2 + cq + c for c in range(co)}}
    xlist, ylist, zlist = ([(index[k, c], r) for k, c, r in table if (k, c) in index]
                           for table in (X_PIECES, Y_PIECES, Z_PIECES))
    route = {**{k: "x" for k in xlist}, **{k: "y" for k in ylist}, **{k: "z" for k in zlist}}
    relays = 2 * len([1 for k in range(2, seqs, 2) for o in (1, 2) if k + o < seqs])
    dma = pltpu.SemaphoreType.DMA
    vmem = pl.BlockSpec(memory_space=pltpu.VMEM)
    hbm = pl.BlockSpec(memory_space=pltpu.HBM)
    result = pl.pallas_call(
        functools.partial(kernel, n, groups, seqs, route, xlist, ylist, zlist, cq, co),
        out_shape=pltpu.VMEM((rows, width), BF),
        in_specs=[hbm] * 7,
        out_specs=vmem,
        scratch_shapes=[
            pltpu.VMEM((n,) + key_weight.shape, BF),
            pltpu.VMEM((n,) + value_weight.shape, BF),
            pltpu.VMEM((n,) + query_weight.shape, BF),
            pltpu.VMEM((n,) + out_weight.shape, BF),
            pltpu.VMEM((rows, width), BF),
            pltpu.VMEM((1, HEAD_DIM), F32),
            pltpu.VMEM((1, HEAD_DIM), F32),
            pltpu.VMEM((rows, LANES), F32),
            pltpu.VMEM((rows, LANES), F32),
            pltpu.VMEM((seqs, rows, 2 * kvw), BF),
            pltpu.VMEM((rows, kvw), F32),
            pltpu.VMEM((rows, kvw), F32),
            pltpu.VMEM((rows, qw), F32),
            pltpu.VMEM((qw // LANES, 2 * rows, LANES), BF),
            pltpu.VMEM((rows, qw), BF),
            pltpu.VMEM((KV_HEADS // 2, qw // KV_HEADS // HEAD_DIM * rows, seqs * rows), BF),
            dma((7,)), dma((4,)), dma((4,)),
            dma((chips - 1, 4)), dma((chips - 1, len(xlist))),
            dma((chips - 1, 4)), dma((chips - 1, len(ylist))),
            dma((chips - 1, 4)), dma((chips - 1, len(zlist))),
            dma((chips - 1, 4)), dma((chips - 1, 5)),
            dma((4,)), dma((seqs, 2)), dma((max(1, relays),)), pltpu.SemaphoreType.REGULAR((2,)),
        ],
        compiler_params=pltpu.CompilerParams(
            collective_id=0, has_side_effects=True, vmem_limit_bytes=40 * 2 ** 20),
    )(*[pltpu.with_memory_space_constraint(a, pltpu.HBM) for a in (
        local, key_weight, value_weight, query_weight, out_weight,
        query_gain.reshape(1, HEAD_DIM), key_gain.reshape(1, HEAD_DIM))])
    return result.reshape(1, rows, width)


def solution(mesh):
    in_specs = (
        P(("grp", "dp"), "sp", None),
        P("dp", None),
        P("dp", None),
        P("dp", None),
        P(None, "dp"),
        P(),
        P(),
    )
    out_specs = P(("grp", "dp"), "sp", None)
    body = functools.partial(shards, mesh.shape["dp"], mesh.shape["grp"], mesh.shape["sp"])
    return jax.shard_map(body, mesh=mesh, in_specs=in_specs, out_specs=out_specs, check_vma=False)
```

```python
import functools
import math

import jax
import jax.numpy as jnp
from jax import lax
from jax.experimental import pallas as pl
from jax.experimental.pallas import tpu as pltpu
from jax.sharding import PartitionSpec as P

HEADS = 16
KV_HEADS = 4
HEAD_DIM = 64
GRID_W = 64
LANES = 128

theta_base = 10000.0
norm_eps = 1e-06

BF = jnp.bfloat16
F32 = jnp.float32
MESH = pl.DeviceIdType.MESH


def rotary_tables(start, rows):
    quarter = HEAD_DIM // 4
    lane = lax.broadcasted_iota(jnp.int32, (rows, LANES), 1)
    position = start + lax.broadcasted_iota(jnp.int32, (rows, LANES), 0)
    step = lax.rem(lane, quarter).astype(F32)
    inverse = jnp.exp(step * (-math.log(theta_base) / quarter))
    grid_row = lax.div(position, GRID_W)
    grid_col = lax.rem(position, GRID_W)
    place = jnp.where(lax.rem(lane, 2 * quarter) < quarter, grid_row, grid_col).astype(F32)
    angles = place * inverse
    sine = jnp.sin(angles)
    return jnp.cos(angles), jnp.where(lax.rem(lane, HEAD_DIM) < HEAD_DIM // 2, -sine, sine)


def dot(a, b):
    return jnp.dot(a, b, preferred_element_type=F32)

REACH = (2, 3)
X_PIECES = ((0, 0, 0), (2, 0, 0), (1, 0, 0), (2, 3, 0), (0, 0, 3), (2, 2, 0), (2, 1, 0), (2, 1, 2), (3, 0, 0), (3, 3, 2), (2, 2, 3), (3, 3, 0), (3, 1, 2), (3, 2, 0), (3, 0, 3), (3, 1, 1), (3, 1, 0), (3, 2, 3))
Y_PIECES = ((0, 0, 1), (1, 0, 1), (1, 0, 3), (2, 0, 1), (2, 0, 3), (2, 1, 1), (2, 1, 3), (2, 2, 1), (2, 3, 1), (2, 3, 3), (3, 0, 1), (3, 1, 3), (3, 2, 1), (3, 3, 1), (3, 3, 3))
Z_PIECES = ((0, 0, 2), (1, 0, 2), (2, 0, 2), (2, 2, 2), (2, 3, 2), (3, 0, 2), (3, 2, 2))


def relays_of(seqs):
    return [(which, way, k, o) for which in range(2) for way in (1, -1)
            for k in range(REACH[which], seqs, REACH[which]) for o in range(1, REACH[which] + 1) if k + o < seqs]


def kernel(n, groups, seqs, route, xlist, ylist, zlist, cq, co, tok_h, wk, wv, wq, wo, gq_h, gk_h, out,
           fk, fv, fq, fo, tok, gq, gk, cos, sin, kv, acc_k, acc_v, acc_q, qs, att, probs,
           ls, os_, or_, xs, xr, ys, yr, zs, zr, cs, cr, hs, hr, fs, ready):
    d = lax.axis_index("dp")
    g = lax.axis_index("grp")
    s = lax.axis_index("sp")
    chips = n // 2
    mate = d + 1 - 2 * lax.rem(d, 2)
    full = (fk, fv, fq, fo)
    rows = tok.shape[0]

    loads = []
    for i, (src, dst) in enumerate(((wk, fk.at[d]), (wv, fv.at[d]), (tok_h, tok), (wq, fq.at[d]), (wo, fo.at[d]),
                                    (gq_h, gq), (gk_h, gk))):
        copy = pltpu.make_async_copy(src, dst, ls.at[i])
        copy.start()
        loads.append(copy)

    def hop(j):
        return lax.rem(d + 2 * j, n)

    def back(dev, j):
        return lax.rem(dev + n - 2 * j, n)

    def other(i):
        return i + 1 - 2 * lax.rem(i, 2)

    def inside(i):
        return (i >= 0) & (i < seqs)

    def near(i):
        return jnp.clip(i, 0, seqs - 1)

    e = lax.rem(s, 2)
    colors = (2 * g + e, 2 * other(g) + e, 2 * g + other(e), 2 * other(g) + other(e))
    offsets = tuple(way * o for o in range(max(REACH), 0, -1) for way in (1, -1))

    barrier = pltpu.get_barrier_semaphore()
    for j in range(1, chips):
        pl.semaphore_signal(barrier, inc=1, device_id={"dp": hop(j)}, device_id_type=MESH)
    for i in range(1, groups):
        pl.semaphore_signal(barrier, inc=1, device_id={"grp": lax.rem(g + i, groups)}, device_id_type=MESH)
    count = jnp.int32(chips - 1 + groups - 1 + 1)
    for o in (1, -1):
        def greet(o=o):
            pl.semaphore_signal(barrier, inc=1, device_id={"sp": near(s + o)}, device_id_type=MESH)
        pl.when(inside(s + o))(greet)
        count = count + inside(s + o).astype(jnp.int32)
    pl.semaphore_signal(barrier, inc=1, device_id={"dp": mate}, device_id_type=MESH)

    cos[...], sin[...] = rotary_tables(s * rows, rows)

    waits = []

    def remote(src, dst, ssem, rsem, where):
        return pltpu.make_async_remote_copy(
            src_ref=src, dst_ref=dst, send_sem=ssem, recv_sem=rsem, device_id=where, device_id_type=MESH)

    def arrive(dst, ssem, rsem):
        remote(dst, dst, ssem, rsem, {"dp": mate}).wait_recv()

    pieces = [(0, 0), (1, 0)] + [(2, c) for c in range(cq)] + [(3, c) for c in range(co)]
    cuts = (1, 1, cq, co)

    shelf = [kind if kind < 2 else 2 + 2 * c // cq if kind == 2 else 4 for kind, c in pieces]

    def part(owner, p, start, blocks):
        kind, cut = pieces[p]
        quarter = full[kind].shape[1] // 4
        width = full[kind].shape[2] // cuts[kind]
        ref = full[kind].at[owner]
        if isinstance(start, int):
            return ref.at[pl.ds(start * quarter, blocks * quarter), pl.ds(cut * width, width)]
        return ref.at[pl.ds(pl.multiple_of(start * quarter, 16), blocks * quarter), pl.ds(cut * width, width)]

    def held(owner, p, rel):
        return part(owner, p, colors[rel], 1)

    for copy in loads:
        copy.wait()
    pl.semaphore_wait(barrier, count)

    def vouch(level):
        for i, o in enumerate((1, -1)):
            def tell(i=i, o=o):
                pl.semaphore_signal(ready.at[level - 1, i], inc=1, device_id={"sp": near(s + o)}, device_id_type=MESH)
            pl.when(inside(s + o) & inside(s - level * o))(tell)

    def heard(level):
        for i, o in enumerate((1, -1)):
            def wait(i=i):
                pl.semaphore_wait(ready.at[level - 1, i], 1)
            pl.when(inside(s - o) & inside(s - (level + 1) * o))(wait)

    vouch(1)

    def x_send(index):
        p, rel = xlist[index]
        for j in range(1, chips):
            here = held(d, p, rel)
            remote(here, here, xs.at[j - 1, pieces[p][0]], xr.at[j - 1, index], {"dp": hop(j)}).start()

    def own_send(kind):
        here = full[kind].at[d]
        remote(here, here, os_.at[kind], or_.at[kind], {"dp": mate}).start()

    for index in range(4):
        x_send(index)
    for kind in range(4):
        own_send(kind)
    for index in range(4, len(xlist)):
        x_send(index)

    def step(p, rel):
        way = route[p, rel]
        table, ssem, rsem = {"x": (xlist, xs, xr), "y": (ylist, ys, yr), "z": (zlist, zs, zr)}[way]
        for j in range(1, chips):
            here = held(back(d, j), p, rel)
            arrive(here, ssem.at[j - 1, 0], rsem.at[j - 1, table.index((p, rel))])
            if rel in (0, 1) and route[p, rel + 2] == "z":
                i = zlist.index((p, rel + 2))
                remote(here, here, zs.at[j - 1, pieces[p][0]], zr.at[j - 1, i], {"sp": other(s)}).start()
            if rel in (0, 2) and route[p, rel + 1] == "y":
                i = ylist.index((p, rel + 1))
                remote(here, here, ys.at[j - 1, pieces[p][0]], yr.at[j - 1, i], {"grp": other(g)}).start()
            remote(here, here, cs.at[j - 1, pieces[p][0]], cr.at[j - 1, shelf[p]], {"dp": mate}).start()

    def step_c(kind, lo, hi):
        width = full[kind].shape[2] // cuts[kind]
        for j in range(1, chips):
            arrive(full[kind].at[back(mate, j), :, pl.ds(lo * width, (hi - lo) * width)],
                   cs.at[j - 1, kind], cr.at[j - 1, shelf[pieces.index((kind, lo))]])

    def step_own(kind):
        arrive(full[kind].at[mate], os_.at[kind], or_.at[kind])

    def drain():
        for kind in range(4):
            here = full[kind].at[d]
            remote(here, here, os_.at[kind], or_.at[kind], {"dp": mate}).wait_send()
        for j in range(1, chips):
            for kind in range(4):
                for table, sem in ((xlist, xs), (ylist, ys), (zlist, zs)):
                    blocks = len([1 for q, _ in table if pieces[q][0] == kind])
                    if blocks:
                        here = full[kind].at[d, pl.ds(0, blocks * (full[kind].shape[1] // 4) // cuts[kind])]
                        remote(here, here, sem.at[j - 1, kind], xr.at[0, 0], {"dp": mate}).wait_send()
                here = full[kind].at[d]
                remote(here, here, cs.at[j - 1, kind], cr.at[j - 1, 0], {"dp": mate}).wait_send()
        for i, o in enumerate(offsets):
            uses = [which for which in range(2) if abs(o) <= REACH[which]]
            here = kv.at[s] if len(uses) == 2 else slot(s, uses[0])
            pl.when(inside(s + o))(remote(here, here, hs.at[i], hr.at[0, 0], {"dp": mate}).wait_send)
        for i, (which, way, k, o) in enumerate(relays):
            here = slot(near(s - way * k), which)
            pl.when(inside(s - way * k) & inside(s + way * o))(
                remote(here, here, fs.at[i], hr.at[0, 0], {"dp": mate}).wait_send)

    relays = relays_of(seqs)
    half = kv.shape[2] // 2

    def slot(i, which):
        return kv.at[i, :, pl.ds(which * half, half)]

    known = []

    def meet(level):
        while len(known) < level:
            heard(len(known) + 1)
            if len(known) + 2 < max(REACH):
                vouch(len(known) + 2)
            known.append(level)

    def spread(which):
        meet(REACH[which] - 1)
        here = slot(s, which)
        for i, o in enumerate(offsets):
            if abs(o) <= REACH[which]:
                pl.when(inside(s + o))(
                    remote(here, here, hs.at[i], hr.at[s, which], {"sp": near(s + o)}).start)

    def onward(which, way, k):
        return functools.reduce(lambda a, b: a | b, [
            inside(s + way * o) for i, w, kk, o in relays if (i, w, kk) == (which, way, k)])

    def take(which, way, k):
        source = near(s - way * k)
        arrive(slot(source, which), hs.at[0], hr.at[source, which])

    def relayed(which, way, k):
        return bool([1 for i, w, kk, o in relays if (i, w, kk) == (which, way, k)])

    def relay(which):
        for k in range(REACH[which], seqs, REACH[which]):
            for way in (1, -1):
                if not relayed(which, way, k):
                    continue
                source = near(s - way * k)
                here = slot(source, which)
                pl.when(inside(s - way * k) & onward(which, way, k))(functools.partial(take, which, way, k))
                for i, (kind, w, kk, o) in enumerate(relays):
                    if (kind, w, kk) == (which, way, k):
                        pl.when(inside(s - way * k) & inside(s + way * o))(
                            remote(here, here, fs.at[i], hr.at[source, which], {"sp": near(s + way * o)}).start)

    def collect(which):
        for k in range(1, seqs):
            for way in (1, -1):
                need = inside(s - way * k)
                if relayed(which, way, k):
                    need = need & jnp.logical_not(onward(which, way, k))
                pl.when(need)(functools.partial(take, which, way, k))

    depth = fq.shape[1]

    def columns(owner):
        return pl.ds(pl.multiple_of(owner * depth, LANES), depth)

    def first(acc, ref):
        acc[...] = dot(tok[:, columns(d)], ref[d])

    def more(acc, ref, owner):
        acc[...] += dot(tok[:, columns(owner)], ref[owner])

    first(acc_k, fk)
    first(acc_v, fv)
    first(acc_q, fq)

    lane = lax.broadcasted_iota(jnp.int32, (rows, LANES), 1)
    low_head = lane < HEAD_DIM
    square_r = lax.broadcasted_iota(jnp.int32, (LANES, LANES), 0)
    square_c = lax.broadcasted_iota(jnp.int32, (LANES, LANES), 1)
    same_head = jnp.where(square_r // HEAD_DIM == square_c // HEAD_DIM, 1.0, 0.0).astype(BF)

    twice_head = jnp.concatenate([same_head] * 2, axis=0)

    def halves(a, b):
        middle = a.shape[0] // 32 * 16
        return jnp.concatenate([dot(a[:middle], b), dot(a[middle:], b)], axis=0)

    gain_k = jnp.concatenate([gk[...]] * 2, axis=1)
    gain_q = jnp.concatenate([gq[...]] * 2, axis=1) * HEAD_DIM ** (-0.5)

    def norm_rotate(acc, tiles_, gain):
        raw = jnp.concatenate([acc[:, pl.ds(t * LANES, LANES)] for t in tiles_], axis=0)
        many = raw.shape[0]
        sq = raw * raw
        high = sq.astype(BF)
        low = (sq - high.astype(F32)).astype(BF)
        total = halves(jnp.concatenate([high, low], axis=1), twice_head)
        scaled = raw * lax.rsqrt(total * (1.0 / HEAD_DIM) + norm_eps) * gain
        lanes = lax.broadcasted_iota(jnp.int32, (many, LANES), 1)
        other = jnp.where(lax.rem(lanes, HEAD_DIM) < HEAD_DIM // 2,
                          pltpu.roll(scaled, LANES - HEAD_DIM // 2, 1), pltpu.roll(scaled, HEAD_DIM // 2, 1))
        again = len(tiles_)
        return scaled * jnp.concatenate([cos[...]] * again, axis=0) + other * jnp.concatenate([sin[...]] * again, axis=0)

    others = [(d, j) for j in range(1, chips)] + [(mate, j) for j in range(1, chips)]

    def finish_k():
        for j in range(1, chips):
            more(acc_k, fk, back(d, j))
        step_c(0, 0, 1)
        for j in range(1, chips):
            more(acc_k, fk, back(mate, j))
        turned = norm_rotate(acc_k, range(half // LANES), gain_k).astype(BF)
        for t in range(half // LANES):
            kv[s, :, pl.ds(t * LANES, LANES)] = turned[t * rows:(t + 1) * rows]

    def finish_v():
        for j in range(1, chips):
            more(acc_v, fv, back(d, j))
        step_c(1, 0, 1)
        for j in range(1, chips):
            more(acc_v, fv, back(mate, j))
        kv[s, :, pl.ds(half, half)] = acc_v[...].astype(BF)

    tiles = fq.shape[2] // LANES
    group = HEADS // KV_HEADS

    def finish_q(part_):
        width = fq.shape[2] // 2
        cols = pl.ds(part_ * width, width)
        step_c(2, part_ * cq // 2, (part_ + 1) * cq // 2)
        for dev, j in others:
            acc_q[:, cols] += dot(tok[:, columns(back(dev, j))], fq[back(dev, j), :, cols])
        mine = range(part_ * tiles // 2, (part_ + 1) * tiles // 2)
        turned = norm_rotate(acc_q, mine, gain_q)
        swapped = pltpu.roll(turned, HEAD_DIM, 1)
        for i, t in enumerate(mine):
            here, there = turned[i * rows:(i + 1) * rows], swapped[i * rows:(i + 1) * rows]
            if (2 * t // group) % 2 == 0:
                one, two = jnp.where(low_head, here, 0.0), jnp.where(low_head, there, 0.0)
            else:
                one, two = jnp.where(low_head, 0.0, there), jnp.where(low_head, 0.0, here)
            qs[t, pl.ds(0, rows), :] = one.astype(BF)
            qs[t, pl.ds(rows, rows), :] = two.astype(BF)

    def soft(h):
        base = (h // 2) * LANES
        keys = kv[:, :, pl.ds(base, LANES)].reshape(seqs * rows, LANES)
        lo, count = h * tiles // KV_HEADS, tiles // KV_HEADS
        asked = qs[lo:lo + count].reshape(count * 2 * rows, LANES)
        blocks = 4
        size = count * 2 * rows // blocks
        def score(i):
            return lax.dot_general(asked[i * size:(i + 1) * size], keys, (((1,), (1,)), ((), ())),
                                   preferred_element_type=F32)

        following = score(0)
        for i in range(blocks):
            scores = following
            if i + 1 < blocks:
                following = score(i + 1)
            top = jnp.max(scores, axis=-1, keepdims=True)
            weights = jnp.exp(scores - top)
            inverse = 1.0 / jnp.sum(weights, axis=-1, keepdims=True)
            probs[h, i * size:(i + 1) * size, :] = (weights * inverse).astype(BF)

    def mix(h, weights):
        base = (h // 2) * LANES
        lo, count = h * tiles // KV_HEADS, tiles // KV_HEADS
        values = kv[:, :, pl.ds(half + base, LANES)].reshape(seqs * rows, LANES)
        mixed = halves(weights, values)
        for i in range(count):
            one, two = mixed[2 * i * rows:(2 * i + 1) * rows], mixed[(2 * i + 1) * rows:(2 * i + 2) * rows]
            if h % 2 == 0:
                two = pltpu.roll(two, HEAD_DIM, 1)
            else:
                one = pltpu.roll(one, HEAD_DIM, 1)
            att[:, pl.ds((lo + i) * LANES, LANES)] = jnp.where(low_head, one, two).astype(BF)

    def blend(h):
        mix(h, probs[h])

    def project(owner, lo, hi):
        width = fo.shape[2]
        size = (hi - lo) * (width // co)
        offset = lo * (width // co)
        out[:, pl.ds(pl.multiple_of(owner * width + offset, LANES), size)] = dot(
            att[...], fo[owner, :, pl.ds(offset, size)]).astype(BF)

    Q = [2 + c for c in range(cq)]
    O = [2 + cq + c for c in range(co)]
    def q(i, rel):
        step(Q[i], rel)


    def od(i, rel):
        if i < co:
            step(O[i], rel)

    step(0, 0)
    meet(1)
    q(0, 0)
    step_own(2)
    more(acc_q, fq, mate)
    step(1, 0)
    q(3, 0)
    step(0, 1)
    q(0, 2)
    step_own(0)
    more(acc_k, fk, mate)
    step_own(1)
    more(acc_v, fv, mate)
    step(0, 3)
    step(1, 2)
    step(0, 2)
    finish_k()
    spread(0)
    q(2, 0)
    q(3, 2)
    q(1, 2)
    step(1, 1)
    q(0, 3)
    relay(0)
    q(1, 0)
    step(1, 3)
    finish_v()
    spread(1)
    q(2, 3)
    od(0, 0)
    od(3, 0)
    q(0, 1)
    q(1, 3)
    q(2, 2)
    q(3, 1)
    q(1, 1)
    q(3, 3)
    od(3, 2)
    q(2, 1)
    finish_q(0)
    finish_q(1)
    od(1, 2)
    od(2, 0)
    relay(1)
    collect(0)
    soft(0)
    soft(2)
    soft(1)
    od(3, 1)
    soft(3)
    collect(1)
    blend(2)
    blend(0)
    od(0, 3)
    od(0, 1)
    od(3, 3)
    od(0, 2)
    od(1, 1)
    blend(1)
    od(2, 3)
    od(2, 1)
    od(1, 3)
    od(1, 0)
    blend(3)
    od(2, 2)
    project(d, 0, co)
    step_own(3)
    project(mate, 0, co)
    [project(back(d, j), 0, co) for j in range(1, chips)]
    step_c(3, 0, co)
    for j in range(1, chips):
        project(back(mate, j), 0, co)
    drain()


def shards(n, groups, seqs, tokens, query_weight, key_weight, value_weight, out_weight, query_gain, key_gain):
    rows, width = tokens.shape[1], tokens.shape[2]
    local = tokens.reshape(rows, width)
    chips = n // 2
    kvw, qw = key_weight.shape[1], query_weight.shape[1]
    cq = 4
    co = max(1, min(4, out_weight.shape[1] // LANES))
    pieces = 2 + cq + co
    index = {(0, 0): 0, (1, 0): 1, **{(2, c): 2 + c for c in range(cq)}, **{(3, c): 2 + cq + c for c in range(co)}}
    xlist, ylist, zlist = ([(index[k, c], r) for k, c, r in table if (k, c) in index]
                           for table in (X_PIECES, Y_PIECES, Z_PIECES))
    route = {**{k: "x" for k in xlist}, **{k: "y" for k in ylist}, **{k: "z" for k in zlist}}
    dma = pltpu.SemaphoreType.DMA
    vmem = pl.BlockSpec(memory_space=pltpu.VMEM)
    hbm = pl.BlockSpec(memory_space=pltpu.HBM)
    result = pl.pallas_call(
        functools.partial(kernel, n, groups, seqs, route, xlist, ylist, zlist, cq, co),
        out_shape=pltpu.VMEM((rows, width), BF),
        in_specs=[hbm] * 7,
        out_specs=vmem,
        scratch_shapes=[
            pltpu.VMEM((n,) + key_weight.shape, BF),
            pltpu.VMEM((n,) + value_weight.shape, BF),
            pltpu.VMEM((n,) + query_weight.shape, BF),
            pltpu.VMEM((n,) + out_weight.shape, BF),
            pltpu.VMEM((rows, width), BF),
            pltpu.VMEM((1, HEAD_DIM), F32),
            pltpu.VMEM((1, HEAD_DIM), F32),
            pltpu.VMEM((rows, LANES), F32),
            pltpu.VMEM((rows, LANES), F32),
            pltpu.VMEM((seqs, rows, 2 * kvw), BF),
            pltpu.VMEM((rows, kvw), F32),
            pltpu.VMEM((rows, kvw), F32),
            pltpu.VMEM((rows, qw), F32),
            pltpu.VMEM((qw // LANES, 2 * rows, LANES), BF),
            pltpu.VMEM((rows, qw), BF),
            pltpu.VMEM((KV_HEADS, qw // KV_HEADS // HEAD_DIM * rows, seqs * rows), BF),
            dma((7,)), dma((4,)), dma((4,)),
            dma((chips - 1, 4)), dma((chips - 1, len(xlist))),
            dma((chips - 1, 4)), dma((chips - 1, len(ylist))),
            dma((chips - 1, 4)), dma((chips - 1, len(zlist))),
            dma((chips - 1, 4)), dma((chips - 1, 5)),
            dma((2 * max(REACH),)), dma((seqs, 2)), dma((max(1, len(relays_of(seqs))),)),
            pltpu.SemaphoreType.REGULAR((max(REACH) - 1, 2)),
        ],
        compiler_params=pltpu.CompilerParams(
            collective_id=0, has_side_effects=True, vmem_limit_bytes=40 * 2 ** 20),
    )(*[pltpu.with_memory_space_constraint(a, pltpu.HBM) for a in (
        local, key_weight, value_weight, query_weight, out_weight,
        query_gain.reshape(1, HEAD_DIM), key_gain.reshape(1, HEAD_DIM))])
    return result.reshape(1, rows, width)


def solution(mesh):
    in_specs = (
        P(("grp", "dp"), "sp", None),
        P("dp", None),
        P("dp", None),
        P("dp", None),
        P(None, "dp"),
        P(),
        P(),
    )
    out_specs = P(("grp", "dp"), "sp", None)
    body = functools.partial(shards, mesh.shape["dp"], mesh.shape["grp"], mesh.shape["sp"])
    return jax.shard_map(body, mesh=mesh, in_specs=in_specs, out_specs=out_specs, check_vma=False)
```

```python
import functools
import math

import jax
import jax.numpy as jnp
from jax import lax
from jax.experimental import pallas as pl
from jax.experimental.pallas import tpu as pltpu
from jax.sharding import PartitionSpec as P

HEADS = 16
KV_HEADS = 4
HEAD_DIM = 64
GRID_W = 64
LANES = 128

theta_base = 10000.0
norm_eps = 1e-06

BF = jnp.bfloat16
F32 = jnp.float32
MESH = pl.DeviceIdType.MESH


def rotary_tables(start, rows):
    quarter = HEAD_DIM // 4
    lane = lax.broadcasted_iota(jnp.int32, (rows, LANES), 1)
    position = start + lax.broadcasted_iota(jnp.int32, (rows, LANES), 0)
    step = lax.rem(lane, quarter).astype(F32)
    inverse = jnp.exp(step * (-math.log(theta_base) / quarter))
    grid_row = lax.div(position, GRID_W)
    grid_col = lax.rem(position, GRID_W)
    place = jnp.where(lax.rem(lane, 2 * quarter) < quarter, grid_row, grid_col).astype(F32)
    angles = place * inverse
    sine = jnp.sin(angles)
    return jnp.cos(angles), jnp.where(lax.rem(lane, HEAD_DIM) < HEAD_DIM // 2, -sine, sine)


def dot(a, b):
    return jnp.dot(a, b, preferred_element_type=F32)

REACH = (2, 3)
X_PIECES = ((0, 0, 0), (2, 0, 0), (1, 0, 0), (2, 3, 0), (0, 0, 3), (2, 2, 0), (2, 1, 0), (2, 1, 2), (3, 0, 0), (3, 3, 2), (2, 2, 3), (3, 3, 0), (3, 1, 2), (3, 2, 0), (3, 0, 3), (3, 1, 1), (3, 1, 0), (3, 2, 3))
Y_PIECES = ((0, 0, 1), (1, 0, 1), (1, 0, 3), (2, 0, 1), (2, 0, 3), (2, 1, 1), (2, 1, 3), (2, 2, 1), (2, 3, 1), (2, 3, 3), (3, 0, 1), (3, 1, 3), (3, 2, 1), (3, 3, 1), (3, 3, 3))
Z_PIECES = ((0, 0, 2), (1, 0, 2), (2, 0, 2), (2, 2, 2), (2, 3, 2), (3, 0, 2), (3, 2, 2))


def relays_of(seqs):
    return [(which, way, k, o) for which in range(2) for way in (1, -1)
            for k in range(REACH[which], seqs, REACH[which]) for o in range(1, REACH[which] + 1) if k + o < seqs]


def kernel(n, groups, seqs, route, xlist, ylist, zlist, cq, co, tok_h, wk, wv, wq, wo, gq_h, gk_h, out,
           fk, fv, fq, fo, tok, gq, gk, cos, sin, kv, acc_k, acc_v, acc_q, qs, att, probs,
           ls, os_, or_, ws, xr, yr, zr, cs, cr, hr, fs, ready):
    d = lax.axis_index("dp")
    g = lax.axis_index("grp")
    s = lax.axis_index("sp")
    chips = n // 2
    mate = d + 1 - 2 * lax.rem(d, 2)
    full = (fk, fv, fq, fo)
    rows = tok.shape[0]

    loads = []
    for i, (src, dst) in enumerate(((wk, fk.at[d]), (wv, fv.at[d]), (wq, fq.at[d]), (wo, fo.at[d]), (tok_h, tok),
                                    (gq_h, gq), (gk_h, gk))):
        loads.append(pltpu.make_async_copy(src, dst, ls.at[i]))
    for i in (0, 2, 1, 3, 4, 5, 6):
        loads[i].start()
    there = []

    def need(i):
        if i not in there:
            there.append(i)
            loads[i].wait()

    def hop(j):
        return lax.rem(d + 2 * j, n)

    def back(dev, j):
        return lax.rem(dev + n - 2 * j, n)

    def other(i):
        return i + 1 - 2 * lax.rem(i, 2)

    def inside(i):
        return (i >= 0) & (i < seqs)

    def near(i):
        return jnp.clip(i, 0, seqs - 1)

    e = lax.rem(s, 2)
    colors = (2 * g + e, 2 * other(g) + e, 2 * g + other(e), 2 * other(g) + other(e))
    offsets = tuple(way * o for o in range(max(REACH), 0, -1) for way in (1, -1))

    barrier = pltpu.get_barrier_semaphore()
    for j in range(1, chips):
        pl.semaphore_signal(barrier, inc=1, device_id={"dp": hop(j)}, device_id_type=MESH)
    for i in range(1, groups):
        pl.semaphore_signal(barrier, inc=1, device_id={"grp": lax.rem(g + i, groups)}, device_id_type=MESH)
    count = jnp.int32(chips - 1 + groups - 1 + 1)
    for o in (1, -1):
        def greet(o=o):
            pl.semaphore_signal(barrier, inc=1, device_id={"sp": near(s + o)}, device_id_type=MESH)
        pl.when(inside(s + o))(greet)
        count = count + inside(s + o).astype(jnp.int32)
    pl.semaphore_signal(barrier, inc=1, device_id={"dp": mate}, device_id_type=MESH)

    cos[...], sin[...] = rotary_tables(s * rows, rows)

    waits = []

    def remote(src, dst, ssem, rsem, where):
        return pltpu.make_async_remote_copy(
            src_ref=src, dst_ref=dst, send_sem=ssem, recv_sem=rsem, device_id=where, device_id_type=MESH)

    def arrive(dst, ssem, rsem):
        remote(dst, dst, ssem, rsem, {"dp": mate}).wait_recv()

    pieces = [(0, 0), (1, 0)] + [(2, c) for c in range(cq)] + [(3, c) for c in range(co)]
    cuts = (1, 1, cq, co)

    shelf = [kind if kind < 2 else 2 + 2 * c // cq if kind == 2 else 4 for kind, c in pieces]

    def part(owner, p, start, blocks):
        kind, cut = pieces[p]
        quarter = full[kind].shape[1] // 4
        width = full[kind].shape[2] // cuts[kind]
        ref = full[kind].at[owner]
        if isinstance(start, int):
            return ref.at[pl.ds(start * quarter, blocks * quarter), pl.ds(cut * width, width)]
        return ref.at[pl.ds(pl.multiple_of(start * quarter, 16), blocks * quarter), pl.ds(cut * width, width)]

    def held(owner, p, rel):
        return part(owner, p, colors[rel], 1)

    need(0)
    pl.semaphore_wait(barrier, count)

    def vouch(level):
        for i, o in enumerate((1, -1)):
            def tell(i=i, o=o):
                pl.semaphore_signal(ready.at[level - 1, i], inc=1, device_id={"sp": near(s + o)}, device_id_type=MESH)
            pl.when(inside(s + o) & inside(s - level * o))(tell)

    def heard(level):
        for i, o in enumerate((1, -1)):
            def wait(i=i):
                pl.semaphore_wait(ready.at[level - 1, i], 1)
            pl.when(inside(s - o) & inside(s - (level + 1) * o))(wait)

    vouch(1)

    def x_send(index):
        p, rel = xlist[index]
        need(pieces[p][0])
        for j in range(1, chips):
            here = held(d, p, rel)
            remote(here, here, ws.at[j - 1], xr.at[j - 1, index], {"dp": hop(j)}).start()

    def own_send(kind):
        need(kind)
        here = full[kind].at[d]
        remote(here, here, os_.at[0], or_.at[kind], {"dp": mate}).start()

    for index in range(4):
        x_send(index)
    for kind in range(4):
        own_send(kind)
    for index in range(4, len(xlist)):
        x_send(index)

    def step(p, rel):
        way = route[p, rel]
        table, rsem = {"x": (xlist, xr), "y": (ylist, yr), "z": (zlist, zr)}[way]
        for j in range(1, chips):
            here = held(back(d, j), p, rel)
            arrive(here, ws.at[j - 1], rsem.at[j - 1, table.index((p, rel))])
            if rel in (0, 1) and route[p, rel + 2] == "z":
                i = zlist.index((p, rel + 2))
                remote(here, here, ws.at[j - 1], zr.at[j - 1, i], {"sp": other(s)}).start()
            if rel in (0, 2) and route[p, rel + 1] == "y":
                i = ylist.index((p, rel + 1))
                remote(here, here, ws.at[j - 1], yr.at[j - 1, i], {"grp": other(g)}).start()
            remote(here, here, cs.at[j - 1], cr.at[j - 1, shelf[p]], {"dp": mate}).start()

    def step_c(kind, lo, hi):
        width = full[kind].shape[2] // cuts[kind]
        for j in range(1, chips):
            arrive(full[kind].at[back(mate, j), :, pl.ds(lo * width, (hi - lo) * width)],
                   cs.at[j - 1], cr.at[j - 1, shelf[pieces.index((kind, lo))]])

    def step_own(kind):
        arrive(full[kind].at[mate], os_.at[0], or_.at[kind])

    def drain():
        total = sum(ref.shape[1] * ref.shape[2] for ref in full) // fq.shape[2]
        parts = [a for a in range(1, n + 1) if total % (16 * a) == 0 and total // a <= fq.shape[1]][0]
        here = fq.at[pl.ds(0, parts), pl.ds(0, total // parts)]
        remote(here, here, os_.at[0], or_.at[0], {"dp": mate}).wait_send()
        for j in range(1, chips):
            for sem in (ws, cs):
                remote(here, here, sem.at[j - 1], or_.at[0], {"dp": mate}).wait_send()
        for i, o in enumerate(offsets):
            uses = [which for which in range(2) if abs(o) <= REACH[which]]
            here = kv.at[s] if len(uses) == 2 else slot(s, uses[0])
            pl.when(inside(s + o))(remote(here, here, ls.at[i], hr.at[0, 0], {"dp": mate}).wait_send)
        for i, (which, way, k, o) in enumerate(relays):
            here = slot(near(s - way * k), which)
            pl.when(inside(s - way * k) & inside(s + way * o))(
                remote(here, here, fs.at[i], hr.at[0, 0], {"dp": mate}).wait_send)

    relays = relays_of(seqs)
    half = kv.shape[2] // 2

    def slot(i, which):
        return kv.at[i, :, pl.ds(which * half, half)]

    known = []

    def meet(level):
        while len(known) < level:
            heard(len(known) + 1)
            if len(known) + 2 < max(REACH):
                vouch(len(known) + 2)
            known.append(level)

    def spread(which):
        meet(REACH[which] - 1)
        here = slot(s, which)
        for i, o in enumerate(offsets):
            if abs(o) <= REACH[which]:
                pl.when(inside(s + o))(
                    remote(here, here, ls.at[i], hr.at[s, which], {"sp": near(s + o)}).start)

    def onward(which, way, k):
        return functools.reduce(lambda a, b: a | b, [
            inside(s + way * o) for i, w, kk, o in relays if (i, w, kk) == (which, way, k)])

    def take(which, way, k):
        source = near(s - way * k)
        arrive(slot(source, which), ls.at[0], hr.at[source, which])

    def relayed(which, way, k):
        return bool([1 for i, w, kk, o in relays if (i, w, kk) == (which, way, k)])

    def relay(which):
        for k in range(REACH[which], seqs, REACH[which]):
            for way in (1, -1):
                if not relayed(which, way, k):
                    continue
                source = near(s - way * k)
                here = slot(source, which)
                pl.when(inside(s - way * k) & onward(which, way, k))(functools.partial(take, which, way, k))
                for i, (kind, w, kk, o) in enumerate(relays):
                    if (kind, w, kk) == (which, way, k):
                        pl.when(inside(s - way * k) & inside(s + way * o))(
                            remote(here, here, fs.at[i], hr.at[source, which], {"sp": near(s + way * o)}).start)

    def collect(which):
        for k in range(1, seqs):
            for way in (1, -1):
                need = inside(s - way * k)
                if relayed(which, way, k):
                    need = need & jnp.logical_not(onward(which, way, k))
                pl.when(need)(functools.partial(take, which, way, k))

    depth = fq.shape[1]

    def columns(owner):
        return pl.ds(pl.multiple_of(owner * depth, LANES), depth)

    def first(acc, ref):
        acc[...] = dot(tok[:, columns(d)], ref[d])

    def more(acc, ref, owner):
        acc[...] += dot(tok[:, columns(owner)], ref[owner])

    for i in range(len(loads)):
        need(i)
    first(acc_k, fk)
    first(acc_v, fv)
    first(acc_q, fq)

    lane = lax.broadcasted_iota(jnp.int32, (rows, LANES), 1)
    low_head = lane < HEAD_DIM
    square_r = lax.broadcasted_iota(jnp.int32, (LANES, LANES), 0)
    square_c = lax.broadcasted_iota(jnp.int32, (LANES, LANES), 1)
    same_head = jnp.where(square_r // HEAD_DIM == square_c // HEAD_DIM, 1.0, 0.0).astype(BF)

    twice_head = jnp.concatenate([same_head] * 2, axis=0)

    def halves(a, b):
        middle = a.shape[0] // 32 * 16
        return jnp.concatenate([dot(a[:middle], b), dot(a[middle:], b)], axis=0)

    gain_k = jnp.concatenate([gk[...]] * 2, axis=1)
    gain_q = jnp.concatenate([gq[...]] * 2, axis=1) * HEAD_DIM ** (-0.5)

    def norm_rotate(acc, tiles_, gain):
        raw = jnp.concatenate([acc[:, pl.ds(t * LANES, LANES)] for t in tiles_], axis=0)
        many = raw.shape[0]
        sq = raw * raw
        high = sq.astype(BF)
        low = (sq - high.astype(F32)).astype(BF)
        total = halves(jnp.concatenate([high, low], axis=1), twice_head)
        scaled = raw * lax.rsqrt(total * (1.0 / HEAD_DIM) + norm_eps) * gain
        lanes = lax.broadcasted_iota(jnp.int32, (many, LANES), 1)
        other = jnp.where(lax.rem(lanes, HEAD_DIM) < HEAD_DIM // 2,
                          pltpu.roll(scaled, LANES - HEAD_DIM // 2, 1), pltpu.roll(scaled, HEAD_DIM // 2, 1))
        again = len(tiles_)
        return scaled * jnp.concatenate([cos[...]] * again, axis=0) + other * jnp.concatenate([sin[...]] * again, axis=0)

    others = [(d, j) for j in range(1, chips)] + [(mate, j) for j in range(1, chips)]

    def finish_k():
        for j in range(1, chips):
            more(acc_k, fk, back(d, j))
        step_c(0, 0, 1)
        for j in range(1, chips):
            more(acc_k, fk, back(mate, j))
        turned = norm_rotate(acc_k, range(half // LANES), gain_k).astype(BF)
        for t in range(half // LANES):
            kv[s, :, pl.ds(t * LANES, LANES)] = turned[t * rows:(t + 1) * rows]

    def finish_v():
        for j in range(1, chips):
            more(acc_v, fv, back(d, j))
        step_c(1, 0, 1)
        for j in range(1, chips):
            more(acc_v, fv, back(mate, j))
        kv[s, :, pl.ds(half, half)] = acc_v[...].astype(BF)

    tiles = fq.shape[2] // LANES
    group = HEADS // KV_HEADS

    def finish_q(part_):
        width = fq.shape[2] // 2
        cols = pl.ds(part_ * width, width)
        step_c(2, part_ * cq // 2, (part_ + 1) * cq // 2)
        for dev, j in others:
            acc_q[:, cols] += dot(tok[:, columns(back(dev, j))], fq[back(dev, j), :, cols])
        mine = range(part_ * tiles // 2, (part_ + 1) * tiles // 2)
        turned = norm_rotate(acc_q, mine, gain_q)
        swapped = pltpu.roll(turned, HEAD_DIM, 1)
        for i, t in enumerate(mine):
            here, there = turned[i * rows:(i + 1) * rows], swapped[i * rows:(i + 1) * rows]
            if (2 * t // group) % 2 == 0:
                one, two = jnp.where(low_head, here, 0.0), jnp.where(low_head, there, 0.0)
            else:
                one, two = jnp.where(low_head, 0.0, there), jnp.where(low_head, 0.0, here)
            qs[t, pl.ds(0, rows), :] = one.astype(BF)
            qs[t, pl.ds(rows, rows), :] = two.astype(BF)

    def soft(h):
        base = (h // 2) * LANES
        keys = kv[:, :, pl.ds(base, LANES)].reshape(seqs * rows, LANES)
        lo, count = h * tiles // KV_HEADS, tiles // KV_HEADS
        asked = qs[lo:lo + count].reshape(count * 2 * rows, LANES)
        blocks = 4
        size = count * 2 * rows // blocks
        def score(i):
            return lax.dot_general(asked[i * size:(i + 1) * size], keys, (((1,), (1,)), ((), ())),
                                   preferred_element_type=F32)

        following = score(0)
        for i in range(blocks):
            scores = following
            if i + 1 < blocks:
                following = score(i + 1)
            top = jnp.max(scores, axis=-1, keepdims=True)
            weights = jnp.exp(scores - top)
            inverse = 1.0 / jnp.sum(weights, axis=-1, keepdims=True)
            probs[h, i * size:(i + 1) * size, :] = (weights * inverse).astype(BF)

    def mix(h, weights):
        base = (h // 2) * LANES
        lo, count = h * tiles // KV_HEADS, tiles // KV_HEADS
        values = kv[:, :, pl.ds(half + base, LANES)].reshape(seqs * rows, LANES)
        mixed = halves(weights, values)
        for i in range(count):
            one, two = mixed[2 * i * rows:(2 * i + 1) * rows], mixed[(2 * i + 1) * rows:(2 * i + 2) * rows]
            if h % 2 == 0:
                two = pltpu.roll(two, HEAD_DIM, 1)
            else:
                one = pltpu.roll(one, HEAD_DIM, 1)
            att[:, pl.ds((lo + i) * LANES, LANES)] = jnp.where(low_head, one, two).astype(BF)

    def blend(h):
        mix(h, probs[h])

    def project(owner, lo, hi):
        width = fo.shape[2]
        size = (hi - lo) * (width // co)
        offset = lo * (width // co)
        out[:, pl.ds(pl.multiple_of(owner * width + offset, LANES), size)] = dot(
            att[...], fo[owner, :, pl.ds(offset, size)]).astype(BF)

    Q = [2 + c for c in range(cq)]
    O = [2 + cq + c for c in range(co)]
    def q(i, rel):
        step(Q[i], rel)


    def od(i, rel):
        if i < co:
            step(O[i], rel)

    step(0, 0)
    meet(1)
    q(0, 0)
    step_own(2)
    more(acc_q, fq, mate)
    step(1, 0)
    q(3, 0)
    step(0, 1)
    q(0, 2)
    step_own(0)
    more(acc_k, fk, mate)
    step_own(1)
    more(acc_v, fv, mate)
    step(0, 3)
    step(1, 2)
    step(0, 2)
    finish_k()
    spread(0)
    q(2, 0)
    q(3, 2)
    q(1, 2)
    step(1, 1)
    q(0, 3)
    relay(0)
    q(1, 0)
    step(1, 3)
    finish_v()
    spread(1)
    q(2, 3)
    od(0, 0)
    od(3, 0)
    q(0, 1)
    q(1, 3)
    q(2, 2)
    q(3, 1)
    q(1, 1)
    q(3, 3)
    od(3, 2)
    q(2, 1)
    finish_q(0)
    finish_q(1)
    od(1, 2)
    od(2, 0)
    relay(1)
    collect(0)
    soft(0)
    soft(2)
    soft(1)
    od(3, 1)
    soft(3)
    collect(1)
    blend(2)
    blend(0)
    od(0, 3)
    od(0, 1)
    od(3, 3)
    od(0, 2)
    od(1, 1)
    blend(1)
    od(2, 3)
    od(2, 1)
    od(1, 3)
    od(1, 0)
    blend(3)
    od(2, 2)
    project(d, 0, co)
    step_own(3)
    project(mate, 0, co)
    [project(back(d, j), 0, co) for j in range(1, chips)]
    step_c(3, 0, co)
    for j in range(1, chips):
        project(back(mate, j), 0, co)
    drain()


def shards(n, groups, seqs, tokens, query_weight, key_weight, value_weight, out_weight, query_gain, key_gain):
    rows, width = tokens.shape[1], tokens.shape[2]
    local = tokens.reshape(rows, width)
    chips = n // 2
    kvw, qw = key_weight.shape[1], query_weight.shape[1]
    cq = 4
    co = max(1, min(4, out_weight.shape[1] // LANES))
    pieces = 2 + cq + co
    index = {(0, 0): 0, (1, 0): 1, **{(2, c): 2 + c for c in range(cq)}, **{(3, c): 2 + cq + c for c in range(co)}}
    xlist, ylist, zlist = ([(index[k, c], r) for k, c, r in table if (k, c) in index]
                           for table in (X_PIECES, Y_PIECES, Z_PIECES))
    route = {**{k: "x" for k in xlist}, **{k: "y" for k in ylist}, **{k: "z" for k in zlist}}
    dma = pltpu.SemaphoreType.DMA
    vmem = pl.BlockSpec(memory_space=pltpu.VMEM)
    hbm = pl.BlockSpec(memory_space=pltpu.HBM)
    result = pl.pallas_call(
        functools.partial(kernel, n, groups, seqs, route, xlist, ylist, zlist, cq, co),
        out_shape=pltpu.VMEM((rows, width), BF),
        in_specs=[hbm] * 7,
        out_specs=vmem,
        scratch_shapes=[
            pltpu.VMEM((n,) + key_weight.shape, BF),
            pltpu.VMEM((n,) + value_weight.shape, BF),
            pltpu.VMEM((n,) + query_weight.shape, BF),
            pltpu.VMEM((n,) + out_weight.shape, BF),
            pltpu.VMEM((rows, width), BF),
            pltpu.VMEM((1, HEAD_DIM), F32),
            pltpu.VMEM((1, HEAD_DIM), F32),
            pltpu.VMEM((rows, LANES), F32),
            pltpu.VMEM((rows, LANES), F32),
            pltpu.VMEM((seqs, rows, 2 * kvw), BF),
            pltpu.VMEM((rows, kvw), F32),
            pltpu.VMEM((rows, kvw), F32),
            pltpu.VMEM((rows, qw), F32),
            pltpu.VMEM((qw // LANES, 2 * rows, LANES), BF),
            pltpu.VMEM((rows, qw), BF),
            pltpu.VMEM((KV_HEADS, qw // KV_HEADS // HEAD_DIM * rows, seqs * rows), BF),
            dma((7,)), dma((1,)), dma((4,)), dma((chips - 1,)), dma((chips - 1, len(xlist))),
            dma((chips - 1, len(ylist))), dma((chips - 1, len(zlist))), dma((chips - 1,)), dma((chips - 1, 5)),
            dma((seqs, 2)), dma((max(1, len(relays_of(seqs))),)),
            pltpu.SemaphoreType.REGULAR((max(REACH) - 1, 2)),
        ],
        compiler_params=pltpu.CompilerParams(
            collective_id=0, has_side_effects=True, vmem_limit_bytes=40 * 2 ** 20),
    )(*[pltpu.with_memory_space_constraint(a, pltpu.HBM) for a in (
        local, key_weight, value_weight, query_weight, out_weight,
        query_gain.reshape(1, HEAD_DIM), key_gain.reshape(1, HEAD_DIM))])
    return result.reshape(1, rows, width)


def solution(mesh):
    in_specs = (
        P(("grp", "dp"), "sp", None),
        P("dp", None),
        P("dp", None),
        P("dp", None),
        P(None, "dp"),
        P(),
        P(),
    )
    out_specs = P(("grp", "dp"), "sp", None)
    body = functools.partial(shards, mesh.shape["dp"], mesh.shape["grp"], mesh.shape["sp"])
    return jax.shard_map(body, mesh=mesh, in_specs=in_specs, out_specs=out_specs, check_vma=False)
```

```python
import functools
import math

import jax
import jax.numpy as jnp
from jax import lax
from jax.experimental import pallas as pl
from jax.experimental.pallas import tpu as pltpu
from jax.sharding import PartitionSpec as P

HEADS = 16
KV_HEADS = 4
HEAD_DIM = 64
GRID_W = 64
LANES = 128

theta_base = 10000.0
norm_eps = 1e-06

BF = jnp.bfloat16
F32 = jnp.float32
MESH = pl.DeviceIdType.MESH


def rotary_tables(start, rows):
    quarter = HEAD_DIM // 4
    lane = lax.broadcasted_iota(jnp.int32, (rows, LANES), 1)
    position = start + lax.broadcasted_iota(jnp.int32, (rows, LANES), 0)
    step = lax.rem(lane, quarter).astype(F32)
    inverse = jnp.exp(step * (-math.log(theta_base) / quarter))
    grid_row = lax.div(position, GRID_W)
    grid_col = lax.rem(position, GRID_W)
    place = jnp.where(lax.rem(lane, 2 * quarter) < quarter, grid_row, grid_col).astype(F32)
    angles = place * inverse
    sine = jnp.sin(angles)
    return jnp.cos(angles), jnp.where(lax.rem(lane, HEAD_DIM) < HEAD_DIM // 2, -sine, sine)


def dot(a, b):
    return jnp.dot(a, b, preferred_element_type=F32)

REACH = (2, 3)
X_PIECES = ((0, 0, 0), (2, 0, 0), (1, 0, 0), (2, 3, 0), (0, 0, 3), (2, 2, 0), (2, 1, 0), (2, 1, 2), (3, 0, 0), (3, 3, 2), (2, 2, 3), (3, 3, 0), (3, 1, 2), (3, 2, 0), (3, 0, 3), (3, 1, 1), (3, 1, 0), (3, 2, 3))
Y_PIECES = ((0, 0, 1), (1, 0, 1), (1, 0, 3), (2, 0, 1), (2, 0, 3), (2, 1, 1), (2, 1, 3), (2, 2, 1), (2, 3, 1), (2, 3, 3), (3, 0, 1), (3, 1, 3), (3, 2, 1), (3, 3, 1), (3, 3, 3))
Z_PIECES = ((0, 0, 2), (1, 0, 2), (2, 0, 2), (2, 2, 2), (2, 3, 2), (3, 0, 2), (3, 2, 2))


def relays_of(seqs):
    return [(which, way, k, o) for which in range(2) for way in (1, -1)
            for k in range(REACH[which], seqs, REACH[which]) for o in range(1, REACH[which] + 1) if k + o < seqs]


def kernel(n, groups, seqs, route, xlist, ylist, zlist, cq, co, tok_h, wk, wv, wq, wo, gq_h, gk_h, out,
           fk, fv, fq, fo, tok, gq, gk, cos, sin, kv, acc_k, acc_v, acc_q, acc_o, qs, att, probs,
           ls, os_, or_, ws, xr, yr, zr, cs, cr, hr, fs, ready):
    d = lax.axis_index("dp")
    g = lax.axis_index("grp")
    s = lax.axis_index("sp")
    chips = n // 2
    mate = d + 1 - 2 * lax.rem(d, 2)
    full = (fk, fv, fq, fo)
    rows = tok.shape[0]

    loads = []
    for i, (src, dst) in enumerate(((wk, fk.at[d]), (wv, fv.at[d]), (wq, fq.at[d]), (wo, fo.at[d]), (tok_h, tok),
                                    (gq_h, gq), (gk_h, gk))):
        loads.append(pltpu.make_async_copy(src, dst, ls.at[i]))
    for i in (0, 2, 1, 3, 4, 5, 6):
        loads[i].start()
    there = []

    def need(i):
        if i not in there:
            there.append(i)
            loads[i].wait()

    def hop(j):
        return lax.rem(d + 2 * j, n)

    def back(dev, j):
        return lax.rem(dev + n - 2 * j, n)

    def other(i):
        return i + 1 - 2 * lax.rem(i, 2)

    def inside(i):
        return (i >= 0) & (i < seqs)

    def near(i):
        return jnp.clip(i, 0, seqs - 1)

    e = lax.rem(s, 2)
    colors = (2 * g + e, 2 * other(g) + e, 2 * g + other(e), 2 * other(g) + other(e))
    offsets = tuple(way * o for o in range(max(REACH), 0, -1) for way in (1, -1))

    barrier = pltpu.get_barrier_semaphore()
    for j in range(1, chips):
        pl.semaphore_signal(barrier, inc=1, device_id={"dp": hop(j)}, device_id_type=MESH)
    for i in range(1, groups):
        pl.semaphore_signal(barrier, inc=1, device_id={"grp": lax.rem(g + i, groups)}, device_id_type=MESH)
    count = jnp.int32(chips - 1 + groups - 1 + 1)
    for o in (1, -1):
        def greet(o=o):
            pl.semaphore_signal(barrier, inc=1, device_id={"sp": near(s + o)}, device_id_type=MESH)
        pl.when(inside(s + o))(greet)
        count = count + inside(s + o).astype(jnp.int32)
    pl.semaphore_signal(barrier, inc=1, device_id={"dp": mate}, device_id_type=MESH)

    cos[...], sin[...] = rotary_tables(s * rows, rows)

    waits = []

    def remote(src, dst, ssem, rsem, where):
        return pltpu.make_async_remote_copy(
            src_ref=src, dst_ref=dst, send_sem=ssem, recv_sem=rsem, device_id=where, device_id_type=MESH)

    def arrive(dst, ssem, rsem):
        remote(dst, dst, ssem, rsem, {"dp": mate}).wait_recv()

    pieces = [(0, 0), (1, 0)] + [(2, c) for c in range(cq)] + [(3, c) for c in range(co)]
    cuts = (1, 1, cq, co)

    shelf = [kind if kind < 2 else 2 + 2 * c // cq if kind == 2 else 4 for kind, c in pieces]

    def part(owner, p, start, blocks):
        kind, cut = pieces[p]
        quarter = full[kind].shape[1] // 4
        width = full[kind].shape[2] // cuts[kind]
        ref = full[kind].at[owner]
        if isinstance(start, int):
            return ref.at[pl.ds(start * quarter, blocks * quarter), pl.ds(cut * width, width)]
        return ref.at[pl.ds(pl.multiple_of(start * quarter, 16), blocks * quarter), pl.ds(cut * width, width)]

    def held(owner, p, rel):
        return part(owner, p, colors[rel], 1)

    need(0)
    pl.semaphore_wait(barrier, count)

    def vouch(level):
        for i, o in enumerate((1, -1)):
            def tell(i=i, o=o):
                pl.semaphore_signal(ready.at[level - 1, i], inc=1, device_id={"sp": near(s + o)}, device_id_type=MESH)
            pl.when(inside(s + o) & inside(s - level * o))(tell)

    def heard(level):
        for i, o in enumerate((1, -1)):
            def wait(i=i):
                pl.semaphore_wait(ready.at[level - 1, i], 1)
            pl.when(inside(s - o) & inside(s - (level + 1) * o))(wait)

    vouch(1)

    def x_send(index):
        p, rel = xlist[index]
        need(pieces[p][0])
        for j in range(1, chips):
            here = held(d, p, rel)
            remote(here, here, ws.at[j - 1], xr.at[j - 1, index], {"dp": hop(j)}).start()

    def own_send(kind):
        need(kind)
        here = full[kind].at[d]
        remote(here, here, os_.at[0], or_.at[kind], {"dp": mate}).start()

    for index in range(4):
        x_send(index)
    for kind in range(4):
        own_send(kind)
    for index in range(4, len(xlist)):
        x_send(index)

    def step(p, rel):
        way = route[p, rel]
        table, rsem = {"x": (xlist, xr), "y": (ylist, yr), "z": (zlist, zr)}[way]
        for j in range(1, chips):
            here = held(back(d, j), p, rel)
            arrive(here, ws.at[j - 1], rsem.at[j - 1, table.index((p, rel))])
            if rel in (0, 1) and route[p, rel + 2] == "z":
                i = zlist.index((p, rel + 2))
                remote(here, here, ws.at[j - 1], zr.at[j - 1, i], {"sp": other(s)}).start()
            if rel in (0, 2) and route[p, rel + 1] == "y":
                i = ylist.index((p, rel + 1))
                remote(here, here, ws.at[j - 1], yr.at[j - 1, i], {"grp": other(g)}).start()
            remote(here, here, cs.at[j - 1], cr.at[j - 1, shelf[p]], {"dp": mate}).start()

    def step_c(kind, lo, hi):
        width = full[kind].shape[2] // cuts[kind]
        for j in range(1, chips):
            arrive(full[kind].at[back(mate, j), :, pl.ds(lo * width, (hi - lo) * width)],
                   cs.at[j - 1], cr.at[j - 1, shelf[pieces.index((kind, lo))]])

    def step_own(kind):
        arrive(full[kind].at[mate], os_.at[0], or_.at[kind])

    def drain():
        total = sum(ref.shape[1] * ref.shape[2] for ref in full) // fq.shape[2]
        parts = [a for a in range(1, n + 1) if total % (16 * a) == 0 and total // a <= fq.shape[1]][0]
        here = fq.at[pl.ds(0, parts), pl.ds(0, total // parts)]
        remote(here, here, os_.at[0], or_.at[0], {"dp": mate}).wait_send()
        for j in range(1, chips):
            for sem in (ws, cs):
                remote(here, here, sem.at[j - 1], or_.at[0], {"dp": mate}).wait_send()
        for i, o in enumerate(offsets):
            uses = [which for which in range(2) if abs(o) <= REACH[which]]
            here = kv.at[s] if len(uses) == 2 else slot(s, uses[0])
            pl.when(inside(s + o))(remote(here, here, ls.at[i], hr.at[0, 0], {"dp": mate}).wait_send)
        for i, (which, way, k, o) in enumerate(relays):
            here = slot(near(s - way * k), which)
            pl.when(inside(s - way * k) & inside(s + way * o))(
                remote(here, here, fs.at[i], hr.at[0, 0], {"dp": mate}).wait_send)

    relays = relays_of(seqs)
    half = kv.shape[2] // 2

    def slot(i, which):
        return kv.at[i, :, pl.ds(which * half, half)]

    known = []

    def meet(level):
        while len(known) < level:
            heard(len(known) + 1)
            if len(known) + 2 < max(REACH):
                vouch(len(known) + 2)
            known.append(level)

    def spread(which):
        meet(REACH[which] - 1)
        here = slot(s, which)
        for i, o in enumerate(offsets):
            if abs(o) <= REACH[which]:
                pl.when(inside(s + o))(
                    remote(here, here, ls.at[i], hr.at[s, which], {"sp": near(s + o)}).start)

    def onward(which, way, k):
        return functools.reduce(lambda a, b: a | b, [
            inside(s + way * o) for i, w, kk, o in relays if (i, w, kk) == (which, way, k)])

    def take(which, way, k):
        source = near(s - way * k)
        arrive(slot(source, which), ls.at[0], hr.at[source, which])

    def relayed(which, way, k):
        return bool([1 for i, w, kk, o in relays if (i, w, kk) == (which, way, k)])

    def relay(which):
        for k in range(REACH[which], seqs, REACH[which]):
            for way in (1, -1):
                if not relayed(which, way, k):
                    continue
                source = near(s - way * k)
                here = slot(source, which)
                pl.when(inside(s - way * k) & onward(which, way, k))(functools.partial(take, which, way, k))
                for i, (kind, w, kk, o) in enumerate(relays):
                    if (kind, w, kk) == (which, way, k):
                        pl.when(inside(s - way * k) & inside(s + way * o))(
                            remote(here, here, fs.at[i], hr.at[source, which], {"sp": near(s + way * o)}).start)

    def collect(which):
        for k in range(1, seqs):
            for way in (1, -1):
                need = inside(s - way * k)
                if relayed(which, way, k):
                    need = need & jnp.logical_not(onward(which, way, k))
                pl.when(need)(functools.partial(take, which, way, k))

    depth = fq.shape[1]

    def columns(owner):
        return pl.ds(pl.multiple_of(owner * depth, LANES), depth)

    def first(acc, ref):
        acc[...] = dot(tok[:, columns(d)], ref[d])

    def more(acc, ref, owner):
        acc[...] += dot(tok[:, columns(owner)], ref[owner])

    for i in range(len(loads)):
        need(i)
    first(acc_k, fk)
    first(acc_v, fv)
    first(acc_q, fq)

    lane = lax.broadcasted_iota(jnp.int32, (rows, LANES), 1)
    low_head = lane < HEAD_DIM
    square_r = lax.broadcasted_iota(jnp.int32, (LANES, LANES), 0)
    square_c = lax.broadcasted_iota(jnp.int32, (LANES, LANES), 1)
    same_head = jnp.where(square_r // HEAD_DIM == square_c // HEAD_DIM, 1.0, 0.0).astype(BF)

    twice_head = jnp.concatenate([same_head] * 2, axis=0)

    def halves(a, b):
        middle = a.shape[0] // 32 * 16
        return jnp.concatenate([dot(a[:middle], b), dot(a[middle:], b)], axis=0)

    gain_k = jnp.concatenate([gk[...]] * 2, axis=1)
    gain_q = jnp.concatenate([gq[...]] * 2, axis=1) * HEAD_DIM ** (-0.5)

    def norm_rotate(acc, tiles_, gain):
        raw = jnp.concatenate([acc[:, pl.ds(t * LANES, LANES)] for t in tiles_], axis=0)
        many = raw.shape[0]
        sq = raw * raw
        high = sq.astype(BF)
        low = (sq - high.astype(F32)).astype(BF)
        total = halves(jnp.concatenate([high, low], axis=1), twice_head)
        scaled = raw * lax.rsqrt(total * (1.0 / HEAD_DIM) + norm_eps) * gain
        lanes = lax.broadcasted_iota(jnp.int32, (many, LANES), 1)
        other = jnp.where(lax.rem(lanes, HEAD_DIM) < HEAD_DIM // 2,
                          pltpu.roll(scaled, LANES - HEAD_DIM // 2, 1), pltpu.roll(scaled, HEAD_DIM // 2, 1))
        again = len(tiles_)
        return scaled * jnp.concatenate([cos[...]] * again, axis=0) + other * jnp.concatenate([sin[...]] * again, axis=0)

    others = [(d, j) for j in range(1, chips)] + [(mate, j) for j in range(1, chips)]

    def finish_k():
        for j in range(1, chips):
            more(acc_k, fk, back(d, j))
        step_c(0, 0, 1)
        for j in range(1, chips):
            more(acc_k, fk, back(mate, j))
        turned = norm_rotate(acc_k, range(half // LANES), gain_k).astype(BF)
        for t in range(half // LANES):
            kv[s, :, pl.ds(t * LANES, LANES)] = turned[t * rows:(t + 1) * rows]

    def finish_v():
        for j in range(1, chips):
            more(acc_v, fv, back(d, j))
        step_c(1, 0, 1)
        for j in range(1, chips):
            more(acc_v, fv, back(mate, j))
        kv[s, :, pl.ds(half, half)] = acc_v[...].astype(BF)

    tiles = fq.shape[2] // LANES
    group = HEADS // KV_HEADS

    def finish_q(part_):
        width = fq.shape[2] // 2
        cols = pl.ds(part_ * width, width)
        step_c(2, part_ * cq // 2, (part_ + 1) * cq // 2)
        for dev, j in others:
            acc_q[:, cols] += dot(tok[:, columns(back(dev, j))], fq[back(dev, j), :, cols])
        mine = range(part_ * tiles // 2, (part_ + 1) * tiles // 2)
        turned = norm_rotate(acc_q, mine, gain_q)
        swapped = pltpu.roll(turned, HEAD_DIM, 1)
        for i, t in enumerate(mine):
            here, there = turned[i * rows:(i + 1) * rows], swapped[i * rows:(i + 1) * rows]
            if (2 * t // group) % 2 == 0:
                one, two = jnp.where(low_head, here, 0.0), jnp.where(low_head, there, 0.0)
            else:
                one, two = jnp.where(low_head, 0.0, there), jnp.where(low_head, 0.0, here)
            qs[t, pl.ds(0, rows), :] = one.astype(BF)
            qs[t, pl.ds(rows, rows), :] = two.astype(BF)

    def soft(h):
        base = (h // 2) * LANES
        keys = kv[:, :, pl.ds(base, LANES)].reshape(seqs * rows, LANES)
        lo, count = h * tiles // KV_HEADS, tiles // KV_HEADS
        asked = qs[lo:lo + count].reshape(count * 2 * rows, LANES)
        blocks = 4
        size = count * 2 * rows // blocks
        def score(i):
            return lax.dot_general(asked[i * size:(i + 1) * size], keys, (((1,), (1,)), ((), ())),
                                   preferred_element_type=F32)

        following = score(0)
        for i in range(blocks):
            scores = following
            if i + 1 < blocks:
                following = score(i + 1)
            top = jnp.max(scores, axis=-1, keepdims=True)
            weights = jnp.exp(scores - top)
            inverse = 1.0 / jnp.sum(weights, axis=-1, keepdims=True)
            probs[h, i * size:(i + 1) * size, :] = (weights * inverse).astype(BF)

    def mix(h, weights):
        base = (h // 2) * LANES
        lo, count = h * tiles // KV_HEADS, tiles // KV_HEADS
        values = kv[:, :, pl.ds(half + base, LANES)].reshape(seqs * rows, LANES)
        mixed = halves(weights, values)
        for i in range(count):
            one, two = mixed[2 * i * rows:(2 * i + 1) * rows], mixed[(2 * i + 1) * rows:(2 * i + 2) * rows]
            if h % 2 == 0:
                two = pltpu.roll(two, HEAD_DIM, 1)
            else:
                one = pltpu.roll(one, HEAD_DIM, 1)
            att[:, pl.ds((lo + i) * LANES, LANES)] = jnp.where(low_head, one, two).astype(BF)

    def blend(h):
        mix(h, probs[h])

    def some(owner, chosen):
        size = fo.shape[1] // KV_HEADS
        return sum(dot(att[:, h * size:(h + 1) * size], fo[owner, h * size:(h + 1) * size, :]) for h in chosen)

    def project_first(owner, chosen):
        acc_o[...] = some(owner, chosen)

    def project_rest(owner, chosen):
        width = fo.shape[2]
        out[:, pl.ds(pl.multiple_of(owner * width, LANES), width)] = (acc_o[...] + some(owner, chosen)).astype(BF)

    def project(owner, lo, hi):
        width = fo.shape[2]
        size = (hi - lo) * (width // co)
        offset = lo * (width // co)
        out[:, pl.ds(pl.multiple_of(owner * width + offset, LANES), size)] = dot(
            att[...], fo[owner, :, pl.ds(offset, size)]).astype(BF)

    Q = [2 + c for c in range(cq)]
    O = [2 + cq + c for c in range(co)]
    def q(i, rel):
        step(Q[i], rel)


    def od(i, rel):
        if i < co:
            step(O[i], rel)

    step(0, 0)
    meet(1)
    q(0, 0)
    step_own(2)
    more(acc_q, fq, mate)
    step(1, 0)
    q(3, 0)
    step(0, 1)
    q(0, 2)
    step_own(0)
    more(acc_k, fk, mate)
    step_own(1)
    more(acc_v, fv, mate)
    step(0, 3)
    step(1, 2)
    step(0, 2)
    finish_k()
    spread(0)
    q(2, 0)
    q(3, 2)
    q(1, 2)
    step(1, 1)
    q(0, 3)
    relay(0)
    q(1, 0)
    step(1, 3)
    finish_v()
    spread(1)
    q(2, 3)
    od(0, 0)
    od(3, 0)
    q(0, 1)
    q(1, 3)
    q(2, 2)
    q(3, 1)
    q(1, 1)
    q(3, 3)
    od(3, 2)
    q(2, 1)
    finish_q(0)
    finish_q(1)
    od(1, 2)
    od(2, 0)
    relay(1)
    collect(0)
    soft(0)
    soft(2)
    soft(1)
    od(3, 1)
    soft(3)
    collect(1)
    blend(2)
    blend(0)
    od(0, 3)
    od(0, 1)
    od(3, 3)
    project_first(d, (0, 2))
    od(0, 2)
    od(1, 1)
    blend(1)
    od(2, 3)
    od(2, 1)
    od(1, 3)
    od(1, 0)
    blend(3)
    od(2, 2)
    project_rest(d, (1, 3))
    step_own(3)
    project(mate, 0, co)
    [project(back(d, j), 0, co) for j in range(1, chips)]
    step_c(3, 0, co)
    for j in range(1, chips):
        project(back(mate, j), 0, co)
    drain()


def shards(n, groups, seqs, tokens, query_weight, key_weight, value_weight, out_weight, query_gain, key_gain):
    rows, width = tokens.shape[1], tokens.shape[2]
    local = tokens.reshape(rows, width)
    chips = n // 2
    kvw, qw = key_weight.shape[1], query_weight.shape[1]
    cq = 4
    co = max(1, min(4, out_weight.shape[1] // LANES))
    pieces = 2 + cq + co
    index = {(0, 0): 0, (1, 0): 1, **{(2, c): 2 + c for c in range(cq)}, **{(3, c): 2 + cq + c for c in range(co)}}
    xlist, ylist, zlist = ([(index[k, c], r) for k, c, r in table if (k, c) in index]
                           for table in (X_PIECES, Y_PIECES, Z_PIECES))
    route = {**{k: "x" for k in xlist}, **{k: "y" for k in ylist}, **{k: "z" for k in zlist}}
    dma = pltpu.SemaphoreType.DMA
    vmem = pl.BlockSpec(memory_space=pltpu.VMEM)
    hbm = pl.BlockSpec(memory_space=pltpu.HBM)
    result = pl.pallas_call(
        functools.partial(kernel, n, groups, seqs, route, xlist, ylist, zlist, cq, co),
        out_shape=pltpu.VMEM((rows, width), BF),
        in_specs=[hbm] * 7,
        out_specs=vmem,
        scratch_shapes=[
            pltpu.VMEM((n,) + key_weight.shape, BF),
            pltpu.VMEM((n,) + value_weight.shape, BF),
            pltpu.VMEM((n,) + query_weight.shape, BF),
            pltpu.VMEM((n,) + out_weight.shape, BF),
            pltpu.VMEM((rows, width), BF),
            pltpu.VMEM((1, HEAD_DIM), F32),
            pltpu.VMEM((1, HEAD_DIM), F32),
            pltpu.VMEM((rows, LANES), F32),
            pltpu.VMEM((rows, LANES), F32),
            pltpu.VMEM((seqs, rows, 2 * kvw), BF),
            pltpu.VMEM((rows, kvw), F32),
            pltpu.VMEM((rows, kvw), F32),
            pltpu.VMEM((rows, qw), F32),
            pltpu.VMEM((rows, out_weight.shape[1]), F32),
            pltpu.VMEM((qw // LANES, 2 * rows, LANES), BF),
            pltpu.VMEM((rows, qw), BF),
            pltpu.VMEM((KV_HEADS, qw // KV_HEADS // HEAD_DIM * rows, seqs * rows), BF),
            dma((7,)), dma((1,)), dma((4,)), dma((chips - 1,)), dma((chips - 1, len(xlist))),
            dma((chips - 1, len(ylist))), dma((chips - 1, len(zlist))), dma((chips - 1,)), dma((chips - 1, 5)),
            dma((seqs, 2)), dma((max(1, len(relays_of(seqs))),)),
            pltpu.SemaphoreType.REGULAR((max(REACH) - 1, 2)),
        ],
        compiler_params=pltpu.CompilerParams(
            collective_id=0, has_side_effects=True, vmem_limit_bytes=40 * 2 ** 20),
    )(*[pltpu.with_memory_space_constraint(a, pltpu.HBM) for a in (
        local, key_weight, value_weight, query_weight, out_weight,
        query_gain.reshape(1, HEAD_DIM), key_gain.reshape(1, HEAD_DIM))])
    return result.reshape(1, rows, width)


def solution(mesh):
    in_specs = (
        P(("grp", "dp"), "sp", None),
        P("dp", None),
        P("dp", None),
        P("dp", None),
        P(None, "dp"),
        P(),
        P(),
    )
    out_specs = P(("grp", "dp"), "sp", None)
    body = functools.partial(shards, mesh.shape["dp"], mesh.shape["grp"], mesh.shape["sp"])
    return jax.shard_map(body, mesh=mesh, in_specs=in_specs, out_specs=out_specs, check_vma=False)
```
